32 devices in a mesh: ep: 4 (over y, x), tp: 8 (over z, core).
Axes of the slice: x: 2, y: 2, z: 4, core: 2. Of those that a mesh axis runs over, the one named last changes fastest.
Arguments:
- queries: bfloat16 [4096, 1024], P('ep', 'tp'), may hold values from -12 to 12
- keys: bfloat16 [4096, 1024], P('ep', 'tp'), may hold values from -12 to 12
- values: bfloat16 [4096, 2048], P('ep', 'tp'), may hold values from -6 to 6
- out_gate: bfloat16 [4096, 2048], P('ep', 'tp'), may hold values from -6 to 6
- in_gate: float32 [16, 4096], P('tp', 'ep'), may hold values from -8 to 100
- forget_gate: float32 [16, 4096], P('tp', 'ep'), may hold values from 0 to 16
- out_gain: float32 [2048], P('tp'), may hold values from 0.1 to 1.9
- out_weight: bfloat16 [2048, 4096], P('tp'), may hold values from -0.1875 to 0.1875
- moe_rows: bfloat16 [512, 4096], P('ep'), may hold values from -36 to 36
- moe_gain: float32 [4096], replicated, may hold values from 0.1 to 1.9
- routes: int32 [512, 2], P('ep'), may hold values from 0 to 3, all different within a row; in each aligned block of 128 rows (0 to 127, 128 to 255, ...) at most 96 rows name the same one
- route_weight: float32 [512, 2], P('ep'), may hold values from 0.2 to 1.2
- expert_gate: bfloat16 [4, 4096, 4096], P('ep', None, 'tp'), may hold values from -0.09375 to 0.09375
- expert_up: bfloat16 [4, 4096, 4096], P('ep', None, 'tp'), may hold values from -0.09375 to 0.09375
- expert_down: bfloat16 [4, 4096, 4096], P('ep', 'tp'), may hold values from -0.125 to 0.125
- shared_gate: bfloat16 [4096, 2048], P(None, 'tp'), may hold values from -0.09375 to 0.09375
- shared_up: bfloat16 [4096, 2048], P(None, 'tp'), may hold values from -0.09375 to 0.09375
- shared_down: bfloat16 [2048, 4096], P('tp'), may hold values from -0.1875 to 0.1875
Outputs:
- mixer_out: bfloat16 [4096, 4096], P('ep', 'tp')
- moe_out: bfloat16 [512, 4096], P('ep', 'tp')
The draws below stay inside these ranges and needn't reach their ends.
Inputs may be any that keep to these rules, and one draw needn't show every extreme that they name: `routes`: each row names 2 different experts. Within the 128 rows of one index of ep no expert is named more than 96 times, a bound that some block reaches.
All inputs are finite; a program needn't handle non-finite values.
Results may differ from the reference program's by a relative error of at most 0.019.
Values may be sent and summed in bfloat16 or wider, within the bound.
A program may use at most 128 MiB of HBM per device.

```python
import math
import jax
import jax.numpy as jnp
import numpy as np
from jax import lax

D = 4096
CELL_HEADS = 16
DK = 64
DV = 128
BLK = 64
TA_DEV = 1024
FE = 4096
FS = 2048
TOPK = 2
TB_DEV = 128
HW = 2048
SEQUENCE_TOKENS = 4096
TOKB = 512
EXPERTS = 4
CAP = 96
N_EP = 4
N_TP = 8


def draw_forget_gate(key, part):
    split_random_keys = jax.random.split(jax.random.fold_in(key, 11), 7)
    slow_share = 0.5
    slow_head = jax.random.bernoulli(split_random_keys[0], slow_share, (CELL_HEADS, 1))
    token_position = jnp.arange(SEQUENCE_TOKENS)
    slow_total = jnp.exp(jax.random.uniform(split_random_keys[1], (CELL_HEADS, 1), minval=jnp.log(0.15), maxval=jnp.log(0.5)))
    slow_rate = slow_total / SEQUENCE_TOKENS
    fast_rate = 1.0 / jnp.exp(jax.random.uniform(split_random_keys[2], (CELL_HEADS, 1), minval=jnp.log(20.0), maxval=jnp.log(60.0)))
    forget_decay_speed = jnp.where(slow_head, slow_rate, fast_rate)
    owner = token_position // TA_DEV
    jitter = jnp.exp(jax.random.uniform(split_random_keys[3], (CELL_HEADS, SEQUENCE_TOKENS // TA_DEV), minval=-0.2, maxval=0.2))
    device_factor = (2.0 ** (owner % 2).astype(jnp.float32))[None, :] * jnp.take(jitter, owner, axis=1)
    noise = jnp.exp(jax.random.uniform(split_random_keys[4], (CELL_HEADS, SEQUENCE_TOKENS), minval=-0.5, maxval=0.5))
    forget_decay_speed = forget_decay_speed * device_factor * noise
    spike_location = jax.random.randint(split_random_keys[5], (CELL_HEADS, 2, 1), 0, SEQUENCE_TOKENS)
    spike_reached = jnp.any(token_position[None, None, :] == spike_location, axis=1)
    spike_penalty = jax.random.uniform(split_random_keys[6], (CELL_HEADS, SEQUENCE_TOKENS), minval=0.2, maxval=0.45)
    forget_decay_speed = jnp.where(spike_reached, -jnp.log(1.0 - spike_penalty), forget_decay_speed)
    return (-jnp.log(jnp.expm1(forget_decay_speed))).astype(jnp.float32)


def draw_in_gate(key, part):
    split_random_keys = jax.random.split(jax.random.fold_in(key, 23), 2)
    return jnp.clip(1.5 * jax.random.normal(split_random_keys[1], (CELL_HEADS, SEQUENCE_TOKENS)), -8.0, 8.0).astype(jnp.float32)


def draw_moe_rows(key, part):
    split_random_keys = jax.random.split(jax.random.fold_in(key, 37), 3)
    row_scale = jnp.exp(jax.random.uniform(split_random_keys[0], (TOKB, 1), minval=jnp.log(0.3), maxval=jnp.log(3.0)))
    col_scale = jnp.exp(jax.random.uniform(split_random_keys[1], (1, D), minval=jnp.log(0.5), maxval=jnp.log(2.0)))
    base_draw = jax.random.normal(split_random_keys[2], (TOKB, D))
    return (jnp.clip(base_draw, -6.0, 6.0) * row_scale * col_scale).astype(jnp.bfloat16)


def common_direction(key):
    base = jax.random.normal(jax.random.fold_in(key, 51), (CELL_HEADS, DK))
    unit = base / jnp.sqrt(jnp.sum(base * base, axis=1, keepdims=True))
    return (8.0 * unit).reshape(1, CELL_HEADS * DK)


def draw_queries(key, part):
    noise_key = jax.random.fold_in(key, 61)
    noise = jnp.clip(jax.random.normal(noise_key, (SEQUENCE_TOKENS, CELL_HEADS * DK)), -4.0, 4.0)
    return (noise + common_direction(key)).astype(jnp.bfloat16)


def draw_keys(key, part):
    noise_key = jax.random.fold_in(key, 71)
    noise = jnp.clip(jax.random.normal(noise_key, (SEQUENCE_TOKENS, CELL_HEADS * DK)), -4.0, 4.0)
    return (noise + common_direction(key)).astype(jnp.bfloat16)


def strengthened(drawn, key, source, target, shards_of, factor):
    owner, partner = [(jnp.arange(drawn.shape[axis_at]) // (drawn.shape[axis_at] // shards_of)).reshape([-1 if axis == axis_at else 1 for axis in range(drawn.ndim)]) for axis_at in (source, target)]
    chosen = jax.random.permutation(key, shards_of)[partner]
    strong = (owner == chosen) | (owner == (partner + shards_of // 2) % shards_of)
    return jnp.where(strong, factor * drawn, drawn)


def block_levels(rng, dims, shards, low, high):
    def one(axis_at, parts):
        heights = jax.random.uniform(jax.random.fold_in(jax.random.fold_in(rng, 6), axis_at), (parts,), jnp.float32, low / len(shards), high / len(shards))
        return jnp.repeat(jnp.exp(heights), dims[axis_at] // parts).reshape((-1,) + (1,) * (len(dims) - axis_at - 1))

    level = one(*shards[0])
    for cut in shards[1:]:
        level = level * one(*cut)
    return level


def shared_out(own_key, own, number, rows, count, top, reach, slope):
    ranking = jax.random.permutation(own_key, count)
    crowded, common = portions_of(count, rows * top, reach, slope, True), portions_of(count, rows * top, reach, slope, False)
    places = jnp.arange(count)

    def named(tallies, rotation):
        used = int((tallies > 0).sum())
        fixed = max(1, used // 4)
        shifted = fixed + (places - fixed + rotation * (used - fixed)) % max(1, count - fixed)
        return jnp.zeros((count,), jnp.int32).at[ranking[jnp.where(places < fixed, places, shifted)]].set(jnp.asarray(tallies, jnp.int32))

    tallies = jnp.where(number % 4 == 0, named(crowded, number // 4), named(common, number - number // 4 - 1))
    mixed = jax.random.permutation(jax.random.fold_in(own, 3), count)
    source_of, taker = mixed[0:count // 2 * 2:2], mixed[1:count // 2 * 2:2]
    room = jnp.minimum(tallies[source_of] - 1, reach - tallies[taker]) // 2
    room = jnp.where((source_of == ranking[0]) | (taker == ranking[0]) | (tallies[taker] == 0), 0, jnp.maximum(room, 0))
    shifted = jax.random.randint(jax.random.fold_in(own, 4), (count // 2,), 0, 1 << 20) % (room + 1)
    tallies = tallies.at[source_of].add(-shifted).at[taker].add(shifted)
    labels = jnp.searchsorted(jnp.cumsum(tallies), jnp.arange(rows * top), side="right").astype(jnp.int32)
    table = labels.reshape(top, rows).T
    table = table[jax.random.permutation(jax.random.fold_in(own, 1), rows)]
    rotation = jax.random.randint(jax.random.fold_in(own, 2), (rows, 1), 0, top)
    return jnp.take_along_axis(table, (jnp.arange(top)[None, :] + rotation) % top, axis=1)


def portions_of(amount, total, bound, skew, full):
    weights = [(1 << 20) // math.isqrt(standing ** skew) + 1 for standing in range(1, amount + 1)]
    largest = bound if full else min(bound, max(-(-total // amount), total * weights[0] // sum(weights)))
    least = 1 if total - largest >= amount - 1 else 0
    counts, rest = [largest] + [least] * (amount - 1), total - largest - least * (amount - 1)
    while rest > 0:
        movable = [i for i in range(1, amount) if counts[i] < largest] or [i for i in range(1, amount) if counts[i] < bound]
        mass, remaining = sum([weights[i] for i in movable]), rest
        for i in movable:
            extra = min(bound - counts[i], max(1, remaining * weights[i] // mass), rest)
            counts[i] = counts[i] + extra
            rest = rest - extra
    return np.array(counts)


def centred(rng, shape, spread, bound, cuts=(), kind=jnp.bfloat16):
    loudness = block_levels(rng, shape, cuts, -0.22, 0.18) if cuts else 1.0
    result = jax.random.normal(rng, shape, jnp.float32) * spread * loudness
    return jnp.minimum(jnp.maximum(result, -bound), bound).astype(kind)


def heavy_noise(rng, extent, width, bound, shards, heavy, kind=jnp.bfloat16):
    values = width * jax.random.normal(rng, extent, jnp.float32)
    if shards:
        values = values * block_levels(rng, extent, shards, -0.22, 0.18)
    return jnp.clip(strengthened(values, jax.random.fold_in(rng, 3), *heavy), -bound, bound).astype(kind)


def setup_inputs(seed: int = 0) -> dict:
    arg_keys = jax.random.split(jax.random.key(seed), 19)
    queries = draw_queries(jax.random.fold_in(arg_keys[18], 71), 0)
    keys = draw_keys(jax.random.fold_in(arg_keys[18], 71), 0)
    values = centred(arg_keys[2], (SEQUENCE_TOKENS, HW), 1.0, 6.0, ((0, 4), (1, 8)))
    out_gate = centred(arg_keys[3], (SEQUENCE_TOKENS, HW), 1.0, 6.0, ((0, 4), (1, 8)))
    in_gate = draw_in_gate(jax.random.fold_in(arg_keys[18], 71), 0)
    forget_gate = draw_forget_gate(jax.random.fold_in(arg_keys[18], 71), 0)
    out_gain = jnp.clip(1.0 + 0.18 * jax.random.normal(arg_keys[6], (HW,), jnp.float32), 0.1, 1.9)
    out_weight = heavy_noise(arg_keys[7], (HW, D), HW ** -0.5, 0.1875, ((0, 8),), (0, 1, 8, 2.0))
    moe_rows = draw_moe_rows(jax.random.fold_in(arg_keys[18], 71), 0)
    moe_gain = jnp.clip(1.0 + 0.18 * jax.random.normal(arg_keys[9], (D,), jnp.float32), 0.1, 1.9)
    routes_keys = jax.random.split(jax.random.fold_in(arg_keys[10], 1), TOKB // TB_DEV)
    routes_turns = jax.random.permutation(jax.random.fold_in(arg_keys[10], 3), TOKB // TB_DEV)
    routes = jax.vmap(lambda own, number: shared_out(jax.random.fold_in(arg_keys[10], 2), own, number, TB_DEV, EXPERTS, TOPK, CAP, 2))(routes_keys, routes_turns).reshape((TOKB, TOPK))
    route_weight = jnp.clip(0.2 + 1 * jax.random.uniform(arg_keys[11], (TOKB, TOPK), jnp.float32) ** block_levels(arg_keys[11], (TOKB, TOPK), ((0, 4),), -0.2, 0.2), 0.2, 1.2)
    expert_gate = centred(arg_keys[12], (EXPERTS, D, FE), D ** -0.5, 0.09375, ((0, 4), (2, 8)))
    expert_up = centred(arg_keys[13], (EXPERTS, D, FE), D ** -0.5, 0.09375, ((0, 4), (2, 8)))
    expert_down = heavy_noise(arg_keys[14], (EXPERTS, FE, D), FE ** -0.5, 0.125, ((0, 4), (1, 8)), (1, 2, 8, 2.0))
    shared_gate = centred(arg_keys[15], (D, FS), D ** -0.5, 0.09375, ((1, 8),))
    shared_up = centred(arg_keys[16], (D, FS), D ** -0.5, 0.09375, ((1, 8),))
    shared_down = heavy_noise(arg_keys[17], (FS, D), FS ** -0.5, 0.1875, ((0, 8),), (0, 1, 8, 2.0))
    return {"queries": queries, "keys": keys, "values": values, "out_gate": out_gate, "in_gate": in_gate, "forget_gate": forget_gate, "out_gain": out_gain, "out_weight": out_weight, "moe_rows": moe_rows, "moe_gain": moe_gain, "routes": routes, "route_weight": route_weight, "expert_gate": expert_gate, "expert_up": expert_up, "expert_down": expert_down, "shared_gate": shared_gate, "shared_up": shared_up, "shared_down": shared_down}


highest = lax.Precision.HIGHEST

def group_sum(left_op, right_op, groups):
    group_width = left_op.shape[1] // groups

    def add_group(group_index, running):
        first = (group_index * group_width).astype(jnp.int32)
        left_part = lax.dynamic_slice_in_dim(left_op, first, group_width, 1)
        right_part = lax.dynamic_slice_in_dim(right_op, first, group_width, 0)
        product = jnp.dot(left_part, right_part, preferred_element_type=jnp.float32)
        rounded = lax.optimization_barrier(product.astype(jnp.bfloat16))
        return running + rounded.astype(jnp.float32)
    start_sum = jnp.zeros((left_op.shape[0], right_op.shape[1]), jnp.float32)
    return lax.fori_loop(0, groups, add_group, start_sum)

def memory_head(inputs):
    query_head, key_head, value_head, gate_in, log_forget = inputs
    block_count = query_head.shape[0] // BLK
    scaled_query = (query_head * DK ** (-0.5)).reshape(block_count, BLK, DK)
    key_blocks = key_head.reshape(block_count, BLK, DK)
    value_blocks = value_head.reshape(block_count, BLK, DV)
    gate_blocks = gate_in.reshape(block_count, BLK)
    forget_blocks = log_forget.reshape(block_count, BLK)
    causal = jnp.tril(jnp.ones((BLK, BLK), dtype=bool))

    def block_step(state, block_inputs):
        matrix, normal_vec, stab = state
        query_b, key_b, value_b, gate_b, forget_b = block_inputs
        cumulative = jnp.cumsum(forget_b)
        intra = jnp.where(causal, cumulative[:, None] - cumulative[None, :] + gate_b[None, :], -jnp.inf)
        inter = cumulative + stab
        stab_t = jnp.maximum(inter, lax.optimization_barrier(jnp.max(intra, axis=1)))
        scores = jnp.dot(query_b, key_b.T, precision=highest) * jnp.exp(intra - stab_t[:, None])
        scores_low = lax.optimization_barrier(scores.astype(jnp.bfloat16)).astype(jnp.float32)
        inter_weight = jnp.exp(inter - stab_t)
        numer = jnp.dot(scores_low, value_b, precision=highest)
        numer = numer + inter_weight[:, None] * jnp.dot(query_b, matrix.T, precision=highest)
        signed = lax.optimization_barrier(jnp.sum(scores, axis=1)) + inter_weight * jnp.dot(query_b, normal_vec, precision=highest)
        cells = numer / jnp.maximum(jnp.abs(signed), jnp.exp(-stab_t))[:, None]
        block_last = cumulative[-1]
        state_logs = block_last - cumulative + gate_b
        stab_new = jnp.maximum(block_last + stab, jnp.max(state_logs))
        state_weight = jnp.exp(state_logs - stab_new)
        carried = jnp.exp(block_last + stab - stab_new)
        matrix_new = carried * matrix + jnp.dot((value_b * state_weight[:, None]).T, key_b, precision=highest)
        normal_new = carried * normal_vec + jnp.dot(state_weight, key_b, precision=highest)
        return ((matrix_new, normal_new, stab_new), cells)
    start_state = (jnp.zeros((DV, DK), jnp.float32), jnp.zeros((DK,), jnp.float32), jnp.zeros((), jnp.float32))
    _, cells = lax.scan(block_step, start_state, (scaled_query, key_blocks, value_blocks, gate_blocks, forget_blocks))
    return cells.reshape(block_count * BLK, DV)

def reference(queries, keys, values, out_gate, in_gate, forget_gate, out_gain, out_weight, moe_rows, moe_gain, routes, route_weight, expert_gate, expert_up, expert_down, shared_gate, shared_up, shared_down):
    log_forget = jax.nn.log_sigmoid(forget_gate)
    query_heads = queries.astype(jnp.float32).reshape(SEQUENCE_TOKENS, CELL_HEADS, DK).transpose(1, 0, 2)
    key_heads = keys.astype(jnp.float32).reshape(SEQUENCE_TOKENS, CELL_HEADS, DK).transpose(1, 0, 2)
    value_heads = values.astype(jnp.float32).reshape(SEQUENCE_TOKENS, CELL_HEADS, DV).transpose(1, 0, 2)
    cells = lax.map(memory_head, (query_heads, key_heads, value_heads, in_gate, log_forget))
    cells = cells.transpose(1, 0, 2).reshape(SEQUENCE_TOKENS, HW)
    mixed = (cells * jax.nn.sigmoid(out_gate.astype(jnp.float32)) * out_gain).astype(jnp.bfloat16)
    mixer_out = group_sum(mixed, out_weight, N_TP).astype(jnp.bfloat16)
    rows_wide = moe_rows.astype(jnp.float32)
    inverse = lax.rsqrt(lax.optimization_barrier(jnp.mean(rows_wide * rows_wide, axis=1, keepdims=True)) + 1e-06)
    normed = (rows_wide * inverse * moe_gain).astype(jnp.bfloat16)
    flat_routes = routes.reshape(-1).astype(jnp.int32)
    assigned = flat_routes.shape[0]
    per_block = TB_DEV * TOPK
    onehot = (flat_routes[:, None] == jnp.arange(EXPERTS, dtype=jnp.int32)[None, :]).astype(jnp.int32)
    running = jnp.cumsum(onehot.reshape(N_EP, per_block, EXPERTS), axis=1).reshape(assigned, EXPERTS)
    token_position = lax.optimization_barrier(jnp.sum(running * onehot, axis=1)) - 1
    owner_block = jnp.arange(assigned, dtype=jnp.int32) // per_block
    slot_index = (flat_routes * (N_EP * CAP) + owner_block * CAP + token_position).astype(jnp.int32)
    token_of = jnp.arange(assigned, dtype=jnp.int32) // TOPK
    slot_table = jnp.zeros((EXPERTS * N_EP * CAP,), jnp.int32).at[slot_index].set(token_of)
    slot_table = slot_table.reshape(EXPERTS, N_EP * CAP)

    def expert_rows(inputs):
        row_ids, weight_gate, weight_up, weight_down = inputs
        chosen = normed[row_ids]
        gate_val = jnp.dot(chosen, weight_gate, preferred_element_type=jnp.float32)
        up_val = jnp.dot(chosen, weight_up, preferred_element_type=jnp.float32)
        hidden = (jax.nn.silu(gate_val) * up_val).astype(jnp.bfloat16)
        return group_sum(hidden, weight_down, N_TP).astype(jnp.bfloat16)
    results = lax.map(expert_rows, (slot_table, expert_gate, expert_up, expert_down))
    picked = results.reshape(EXPERTS * N_EP * CAP, D)[slot_index].astype(jnp.float32).reshape(TOKB, TOPK, D)
    shared_gate_val = jnp.dot(normed, shared_gate, preferred_element_type=jnp.float32)
    shared_up_val = jnp.dot(normed, shared_up, preferred_element_type=jnp.float32)
    shared_hidden = (jax.nn.silu(shared_gate_val) * shared_up_val).astype(jnp.bfloat16)
    shared_sum = group_sum(shared_hidden, shared_down, N_TP)
    moe_out = (lax.optimization_barrier(jnp.sum(picked * route_weight[:, :, None], axis=1)) + shared_sum).astype(jnp.bfloat16)
    return (mixer_out, moe_out)
```

```python
import functools

import jax
import jax.numpy as jnp
from jax import lax
from jax.experimental import pallas as pl
from jax.experimental.pallas import tpu as pltpu
from jax.sharding import PartitionSpec as P

DK = 64
DV = 128
CH = 128
F32 = jnp.float32
BF16 = jnp.bfloat16
VM = pl.BlockSpec(memory_space=pltpu.VMEM)
ANY = pl.BlockSpec(memory_space=pl.ANY)
MESH = pl.DeviceIdType.MESH
SPLIT = 2


def gate_rows(ig, fg):
    lane = lax.broadcasted_iota(jnp.int32, ig.shape, 1)
    total = jnp.minimum(fg, 0.0) - jnp.log1p(jnp.exp(-jnp.abs(fg)))
    step = 1
    while step < CH:
        total = total + jnp.where(lane >= step, pltpu.roll(total, step, 1), 0.0)
        step *= 2
    level = ig - total
    top = level
    step = 1
    while step < CH:
        top = jnp.maximum(top, jnp.where(lane >= step, pltpu.roll(top, step, 1), -1e30))
        step *= 2
    return total, level, top


def columns_of(parts):
    rows = sum(part.shape[0] for part in parts)
    padded = -(-rows // 128) * 128
    if padded > rows:
        parts = list(parts) + [jnp.zeros((padded - rows, CH), F32)]
    return jnp.concatenate(parts, axis=0).T


def split_bf16(x):
    high = x.astype(BF16)
    return high, (x - high.astype(F32)).astype(BF16)


def weighted_keys(keys, cols, first, heads, chunks):
    lane_head = lax.broadcasted_iota(jnp.int32, keys.shape, 1) // DK
    weight = jnp.broadcast_to(cols[:, first : first + 1], keys.shape)
    for h in range(1, heads):
        at = first + h * chunks
        weight = jnp.where(lane_head == h, jnp.broadcast_to(cols[:, at : at + 1], keys.shape), weight)
    return split_bf16(keys.astype(F32) * weight)


def add_outer(kw, values):
    dims = (((0,), (0,)), ((), ()))
    return lax.dot_general(kw[0], values, dims, preferred_element_type=F32) + lax.dot_general(
        kw[1], values, dims, preferred_element_type=F32
    )


def pick_head(parts, shape, axis):
    head = lax.broadcasted_iota(jnp.int32, shape, axis) // DK
    out = jnp.broadcast_to(parts[0], shape)
    for h in range(1, len(parts)):
        out = jnp.where(head == h, jnp.broadcast_to(parts[h], shape), out)
    return out


def summary(heads, chunks, k_ref, v_ref, gates, out_ref, slot):
    width = heads * DK
    total, level, top = gates
    shape = total.shape
    chunk = lax.broadcasted_iota(jnp.int32, shape, 0) % chunks
    last = jnp.broadcast_to(total[:, CH - 1 : CH], shape)
    suffix = last
    step = 1
    while step < chunks:
        moved = pltpu.roll(suffix, shape[0] - step, 0)
        suffix = suffix + jnp.where(chunk + step < chunks, moved, 0.0)
        step *= 2
    reach = suffix + jnp.broadcast_to(top[:, CH - 1 : CH], shape)
    tops = [
        jnp.max(reach[h * chunks : (h + 1) * chunks], axis=0, keepdims=True) for h in range(heads)
    ]
    weight = [
        jnp.exp(
            level[h * chunks : (h + 1) * chunks] + suffix[h * chunks : (h + 1) * chunks] - tops[h]
        )
        for h in range(heads)
    ]
    cols = columns_of(weight)
    state = jnp.zeros((width, heads * DV + 128), F32)
    for c in range(chunks):
        rows = pl.ds(c * CH, CH)
        kw = weighted_keys(k_ref[rows, :], cols, c, heads, chunks)
        values = jnp.concatenate([v_ref[rows, :], jnp.ones((CH, 128), BF16)], axis=1)
        state = state + add_outer(kw, values)
    out_ref[slot] = jnp.zeros(out_ref.shape[1:], F32)
    out_ref[slot, 0:width, :] = pick_head(
        [state[:, h * DV : (h + 1) * DV] for h in range(heads)], (width, DV), 0
    )
    normal = state[:, heads * DV :].T
    out_ref[slot, width : width + 1, 0:width] = normal[0:1, :]
    for h in range(heads):
        out_ref[slot, width + 1 + h : width + 2 + h, :] = tops[h]
        at = width + 1 + heads + h
        out_ref[slot, at : at + 1, :] = suffix[h * chunks : h * chunks + 1]


def entering_state(heads, pos, sum_ref):
    width = heads * DK
    matrix = jnp.zeros((width, DV), F32)
    normal = jnp.zeros((1, width), F32)
    stab = [jnp.zeros((1, 128), F32) for _ in range(heads)]
    for e in range(sum_ref.shape[0]):
        reached = e < pos
        part = sum_ref.at[e]
        old_w, new_w, new_stab = [], [], []
        for h in range(heads):
            at = width + 1 + h
            carried = part[at + heads : at + heads + 1, :] + stab[h]
            there = part[at : at + 1, :]
            joined = jnp.maximum(carried, there)
            old_w.append(jnp.where(reached, jnp.exp(carried - joined), 1.0))
            new_w.append(jnp.where(reached, jnp.exp(there - joined), 0.0))
            new_stab.append(jnp.where(reached, joined, stab[h]))
        matrix = (
            pick_head(old_w, (width, DV), 0) * matrix
            + pick_head(new_w, (width, DV), 0) * part[0:width, :]
        )
        normal = (
            pick_head([w[:, 0:width] for w in old_w], (1, width), 1) * normal
            + pick_head([w[:, 0:width] for w in new_w], (1, width), 1)
            * part[width : width + 1, 0:width]
        )
        stab = new_stab
    normal_cols = jnp.broadcast_to(normal, (128, width)).T
    return jnp.concatenate([matrix] * heads + [normal_cols], axis=1), stab


def cell_blocks(
    heads, chunks, state, stab, gates, q_ref, k_ref, v_ref, og_ref, gain_ref, out_ref, after
):
    width = heads * DK
    total, level, top = gates
    shape = total.shape
    last = jnp.broadcast_to(total[:, CH - 1 : CH], shape)
    last_top = jnp.broadcast_to(top[:, CH - 1 : CH], shape)
    entering, leaving = [], []
    for h in range(heads):
        now = stab[h]
        for c in range(chunks):
            r = h * chunks + c
            entering.append(now)
            now = last[r : r + 1] + jnp.maximum(now, last_top[r : r + 1])
            leaving.append(now)
    entering = jnp.concatenate(entering, axis=0)
    leaving = jnp.concatenate(leaving, axis=0)
    peak = jnp.maximum(top, entering)
    decay = jnp.exp(last + entering - leaving)
    count = heads * chunks
    cols = columns_of(
        [
            peak,
            jnp.exp(entering - peak),
            jnp.exp(-(total + peak)),
            jnp.exp(last + level - leaving),
        ]
    )
    causal = lax.broadcasted_iota(jnp.int32, (CH, CH), 0) >= lax.broadcasted_iota(
        jnp.int32, (CH, CH), 1
    )
    lane_head = lax.broadcasted_iota(jnp.int32, (CH, width), 1) // DK
    for c in range(chunks):
        rows = pl.ds(c * CH, CH)
        keys = k_ref[rows, :]
        values = v_ref[rows, :]
        queries = q_ref[rows, :] * jnp.asarray(DK**-0.5, BF16)
        high, low = split_bf16(state)
        for h in range(heads):
            r = h * chunks + c
            mine = jnp.where(lane_head == h, queries, jnp.zeros_like(queries))
            raw = lax.dot_general(
                mine, keys, (((1,), (1,)), ((), ())), preferred_element_type=F32
            )
            logs = level[r : r + 1, :] - cols[:, r : r + 1]
            scores = raw * jnp.exp(jnp.where(causal, logs, -jnp.inf))
            inner = jnp.dot(
                scores.astype(BF16), values[:, h * DV : (h + 1) * DV], preferred_element_type=F32
            )
            across = 0.0
            for piece in (high, low):
                rhs = jnp.concatenate(
                    [piece[:, h * DV : (h + 1) * DV], piece[:, heads * DV :]], axis=1
                )
                across = across + jnp.dot(mine, rhs, preferred_element_type=F32)
            inter = cols[:, count + r : count + r + 1]
            signed = jnp.sum(scores, axis=1, keepdims=True) + inter * across[:, DV : DV + 1]
            divisor = jnp.maximum(jnp.abs(signed), cols[:, 2 * count + r : 2 * count + r + 1])
            cells = (inner + inter * across[:, :DV]) * (1.0 / divisor)
            at = slice(h * DV, (h + 1) * DV)
            gate = og_ref[rows, at].astype(F32)
            out_ref[rows, at] = (cells / (1.0 + jnp.exp(-gate)) * gain_ref[:, at]).astype(BF16)
        if c + 1 < chunks:
            kw = weighted_keys(keys, cols, 3 * count + c, heads, chunks)
            scale = pick_head(
                [decay[h * chunks + c : h * chunks + c + 1] for h in range(heads)], (width, 128), 0
            )
            rhs = jnp.concatenate([values, jnp.ones((CH, 128), BF16)], axis=1)
            state = state * jnp.concatenate([scale] * (heads + 1), axis=1) + add_outer(kw, rhs)
        after(c)


def tiles(width, most):
    return min(width, most)


def step_kernel(
    ep_count,
    tp_count,
    side,
    cap,
    q_ref,
    k_ref,
    v_ref,
    og_ref,
    ig_ref,
    fg_ref,
    gain_ref,
    rows_ref,
    mg_ref,
    routes_ref,
    rw_ref,
    ow_hbm,
    eg_hbm,
    eu_hbm,
    ed_hbm,
    sg_hbm,
    su_hbm,
    sd_hbm,
    mixer_out,
    moe_out,
    sums,
    own,
    mixed,
    wcols,
    normed,
    staged,
    arrived,
    eg,
    eu,
    ed,
    sg,
    su,
    sd,
    hidden,
    shared_hidden,
    give,
    take,
    reduced,
    returned,
    shared_own,
    part_out,
    part_in,
    final,
    load_sem,
    wz_s,
    wz_r,
    wx_s,
    wx_r,
    st_s,
    st_r,
    dx_s,
    dx_r,
    dp_s,
    dp_r,
    up_s,
    up_r,
    dn_s,
    dn_r,
    pa_s,
    pa_r,
    pp_s,
    pp_r,
    rt_s,
    rt_r,
    zs_s,
    zs_r,
):
    e, t = lax.axis_index("ep"), lax.axis_index("tp")
    z, core = t // 2, t % 2
    chips = tp_count // 2
    heads = ig_ref.shape[0]
    tok = q_ref.shape[0]
    chunks = tok // CH
    count, depth = rows_ref.shape
    half = depth // 2
    feat = mixer_out.shape[1]
    share = wcols.shape[2]
    slots = ep_count * cap
    group = tp_count // SPLIT
    seg = tok // SPLIT

    def ep_peer(dy, dx):
        deep = ep_count // side
        return ((e // side + dy) % deep) * side + (e % side + dx) % side

    around = [(dy, dx) for dy in range(ep_count // side) for dx in range(side)][1:]
    around = around[::-1]

    def remote(src, dst, send, recv, where):
        return pltpu.make_async_remote_copy(
            src_ref=src, dst_ref=dst, send_sem=send, recv_sem=recv, device_id=where,
            device_id_type=MESH,
        )

    loads = [
        pltpu.make_async_copy(src, dst, load_sem.at[i])
        for i, (src, dst) in enumerate(
            [
                (sg_hbm, sg),
                (su_hbm, su),
                (eg_hbm.at[0], eg),
                (eu_hbm.at[0], eu),
                (ed_hbm.at[0], ed),
                (sd_hbm, sd),
                (
                    ow_hbm.at[
                        pl.ds(pl.multiple_of(e * share, share), share),
                        pl.ds(pl.multiple_of(t * feat, feat), feat),
                    ],
                    wcols.at[t, e],
                ),
            ]
        )
    ]
    barrier = pltpu.get_barrier_semaphore()
    for dy, dx in around:
        pl.semaphore_signal(barrier, inc=1, device_id=(ep_peer(dy, dx), t), device_id_type=MESH)
    for k in range(1, tp_count):
        pl.semaphore_signal(
            barrier, inc=1, device_id=(e, (t + k) % tp_count), device_id_type=MESH
        )
    for copy in loads:
        copy.start()
    pl.semaphore_wait(barrier, ep_count - 1 + tp_count - 1)

    def wz(to, origin):
        return remote(
            ow_hbm.at[
                pl.ds(pl.multiple_of(e * share, share), share),
                pl.ds(pl.multiple_of(to * feat, feat), feat),
            ],
            wcols.at[origin, e],
            wz_s.at[to],
            wz_r.at[origin],
            (e, to),
        )

    for k in range(1, tp_count):
        wz((t + k) % tp_count, t).start()

    def stacked(ref):
        return jnp.concatenate(
            [ref[h : h + 1, c * CH : (c + 1) * CH] for h in range(heads) for c in range(chunks)],
            axis=0,
        )

    gates = gate_rows(stacked(ig_ref), stacked(fg_ref))
    summary(heads, chunks, k_ref, v_ref, gates, sums, e)

    def st(peer, origin):
        return remote(
            sums.at[origin], sums.at[origin], st_s.at[peer], st_r.at[origin], (peer, t)
        )

    for dy, dx in around:
        st(ep_peer(dy, dx), e).start()

    width = tiles(half, 512)
    square = jnp.zeros((count, 1), F32)
    for n in range(0, depth, width):
        wide = rows_ref[:, n : n + width].astype(F32)
        square = square + jnp.sum(wide * wide, axis=1, keepdims=True)
    inverse = lax.rsqrt(square / depth + 1e-06)
    for n in range(0, depth, width):
        wide = rows_ref[:, n : n + width].astype(F32)
        normed[:, n : n + width] = (wide * inverse * mg_ref[:, n : n + width]).astype(BF16)

    lane = lax.broadcasted_iota(jnp.int32, (count, 128), 1)
    topk = routes_ref.shape[1]
    named = [lane == routes_ref[:, k : k + 1] for k in range(topk)]
    member = named[0]
    for k in range(1, topk):
        member = member | named[k]
    earlier = lax.broadcasted_iota(jnp.int32, (count, count), 0) > lax.broadcasted_iota(
        jnp.int32, (count, count), 1
    )
    before = jnp.dot(
        jnp.where(earlier, 1.0, 0.0).astype(BF16),
        jnp.where(member, 1.0, 0.0).astype(BF16),
        preferred_element_type=F32,
    )
    slot_no = lax.broadcasted_iota(jnp.int32, (count, slots), 1)
    place = jnp.zeros((count, slots), F32)
    weight = jnp.zeros((count, slots), F32)
    for k in range(topk):
        ahead = jnp.sum(jnp.where(named[k], before, 0.0), axis=1, keepdims=True)
        target = routes_ref[:, k : k + 1] * cap + ahead.astype(jnp.int32)
        hit = slot_no == target
        place = jnp.where(hit, 1.0, place)
        weight = jnp.where(hit, rw_ref[:, k : k + 1], weight)
    place = place.astype(BF16)
    weight_high, weight_low = split_bf16(weight)

    def stage(side_no):
        for n in range(0, half, width):
            cols = pl.ds(pl.multiple_of(side_no * half + n, width), width)
            moved = lax.dot_general(
                place, normed[:, cols], (((0,), (0,)), ((), ())), preferred_element_type=F32
            ).astype(BF16)
            for x in range(ep_count):
                staged[side_no, x, :, n : n + width] = moved[x * cap : (x + 1) * cap]

    def dx_copy(peer, origin):
        return remote(
            staged.at[core, peer],
            arrived.at[core, origin],
            dx_s.at[peer],
            dx_r.at[origin],
            (peer, t),
        )

    def dp_copy(origin):
        return remote(
            arrived.at[core, origin],
            arrived.at[core, origin],
            dp_s.at[origin],
            dp_r.at[origin],
            (e, 2 * z + 1 - core),
        )

    def dp_other(origin):
        return remote(
            arrived.at[core, origin],
            arrived.at[1 - core, origin],
            dp_s.at[origin],
            dp_r.at[origin],
            (e, 2 * z + 1 - core),
        )

    stage(core)
    for dy, dx in around:
        dx_copy(ep_peer(dy, dx), e).start()
    stage(1 - core)
    for s in range(2):
        arrived[s, e] = staged[s, e]

    loads[0].wait()
    loads[1].wait()
    gate = jnp.dot(normed[...], sg[...], preferred_element_type=F32)
    up = jnp.dot(normed[...], su[...], preferred_element_type=F32)
    shared_hidden[...] = (gate / (1.0 + jnp.exp(-gate)) * up).astype(BF16)

    def line(kind, part, origin, where):
        sems = {"up": (up_s, up_r), "dn": (dn_s, dn_r), "pa": (pa_s, pa_r)}[kind]
        ref = mixed.at[2 * origin + core, pl.ds(part * seg, seg)]
        return remote(
            ref, ref, sems[0].at[part, origin], sems[1].at[part, origin], (e, where)
        )

    def line_other(part, origin):
        ref = mixed.at[2 * origin + 1 - core, pl.ds(part * seg, seg)]
        return remote(
            ref, ref, pa_s.at[part, origin], pa_r.at[part, origin], (e, 2 * z + 1 - core)
        )

    def go_up(part, origin):
        @pl.when(z + 1 < chips)
        def _():
            line("up", part, origin, t + 2).start()

    def go_down(part, origin):
        @pl.when(z > 0)
        def _():
            line("dn", part, origin, t - 2).start()

    def go_across(part, origin):
        line("pa", part, origin, 2 * z + 1 - core).start()

    def after(c):
        if (c + 1) % (chunks // SPLIT) == 0:
            part = (c + 1) // (chunks // SPLIT) - 1
            mixed[t, part * seg : (part + 1) * seg] = own[part * seg : (part + 1) * seg]
            go_up(part, z)
            go_down(part, z)
            go_across(part, z)

    def relay(step):
        for part in range(SPLIT):

            @pl.when(z >= step)
            def _():
                line("up", part, z - step, t - 2).wait_recv()
                go_up(part, z - step)
                go_across(part, z - step)

            @pl.when(z + step < chips)
            def _():
                line("dn", part, z + step, t + 2).wait_recv()
                go_down(part, z + step)
                go_across(part, z + step)

    for dy, dx in around:
        peer = ep_peer(dy, dx)
        st(peer, peer).wait_recv()
    state, stab = entering_state(heads, e, sums)
    cell_blocks(
        heads, chunks, state, stab, gates, q_ref, k_ref, v_ref, og_ref, gain_ref, own, after
    )

    def wx(part, peer, origin):
        ref = wcols.at[pl.ds(part * group, group), origin]
        return remote(ref, ref, wx_s.at[part, peer], wx_r.at[part, origin], (peer, t))

    loads[6].wait()
    for k in range(1, tp_count):
        wz((t + k) % tp_count, (t + k) % tp_count).wait_recv()
    for dy, dx in around:
        wx(0, ep_peer(dy, dx), e).start()

    for dy, dx in around:
        origin = ep_peer(dy, dx)
        dx_copy(origin, origin).wait_recv()
        dp_copy(origin).start()
    for dy, dx in around:
        dp_other(ep_peer(dy, dx)).wait_recv()

    loads[2].wait()
    loads[3].wait()
    units = eg.shape[1]
    tile = tiles(units, 256)

    def both(weights, n):
        return sum(
            jnp.dot(
                arrived[s].reshape(slots, half),
                weights[s * half : (s + 1) * half, n : n + tile],
                preferred_element_type=F32,
            )
            for s in range(2)
        )

    for n in range(0, units, tile):
        gate = both(eg, n)
        up = both(eu, n)
        hidden[:, n : n + tile] = (gate / (1.0 + jnp.exp(-gate)) * up).astype(BF16)
    relay(1)

    loads[4].wait()
    loads[5].wait()

    def pp(block):
        return remote(
            give.at[block], take.at[block], pp_s.at[block], pp_r.at[block],
            (e, 2 * z + 1 - core),
        )

    def products(block, owner):
        cols = pl.ds(pl.multiple_of((2 * block + owner) * feat, feat), feat)
        return (
            jnp.dot(hidden[...], ed[:, cols], preferred_element_type=F32),
            jnp.dot(shared_hidden[...], sd[:, cols], preferred_element_type=F32),
        )

    for block in range(chips):
        routed, common = products(block, 1 - core)
        give[block, 0:slots] = routed.astype(BF16)
        give[block, slots:] = common.astype(BF16)
        pp(block).start()
    for block in range(chips):
        routed, common = products(block, core)
        pp(block).wait_recv()
        total = (routed + take[block, 0:slots].astype(F32)).astype(BF16)
        for x in range(ep_count):
            reduced[block, x] = total[x * cap : (x + 1) * cap]
        shared_own[block] = common + take[block, slots:].astype(F32)

    def rt(peer, origin):
        return remote(
            reduced.at[:, peer], returned.at[:, origin], rt_s.at[peer], rt_r.at[origin], (peer, t)
        )

    for dy, dx in around:
        rt(ep_peer(dy, dx), e).start()
    for block in range(chips):
        returned[block, e] = reduced[block, e]
    for dy, dx in around:
        wx(1, ep_peer(dy, dx), e).start()
    for step in range(2, chips):
        relay(step)

    for dy, dx in around:
        origin = ep_peer(dy, dx)
        rt(origin, origin).wait_recv()

    def zs(to, origin):
        return remote(
            part_out.at[to], part_in.at[origin], zs_s.at[to], zs_r.at[origin], (e, 2 * to + core)
        )

    for block in range(chips):
        results = returned[block].reshape(slots, feat)
        total = (
            jnp.dot(weight_high, results, preferred_element_type=F32)
            + jnp.dot(weight_low, results, preferred_element_type=F32)
            + shared_own[block]
        )
        part_out[block] = total.astype(BF16)

        @pl.when(z == block)
        def _():
            final[...] = total

    for k in range(1, chips):
        zs((z + k) % chips, z).start()

    for part in range(SPLIT):
        for dy, dx in around:
            origin = ep_peer(dy, dx)
            wx(part, origin, origin).wait_recv()
    for part in range(SPLIT):
        for origin in range(chips):
            line_other(part, origin).wait_recv()
    step_rows = tiles(tok, 256)

    @pl.loop(0, tok // step_rows)
    def _(i):
        rows = pl.ds(pl.multiple_of(i * step_rows, step_rows), step_rows)
        total = 0.0
        for b in range(tp_count):
            total = total + jnp.dot(
                mixed[b, rows],
                wcols[b].reshape(ep_count * share, feat),
                preferred_element_type=F32,
            )
        mixer_out[rows, :] = total.astype(BF16)

    total = final[...]
    for k in range(1, chips):
        origin = (z + k) % chips
        zs(origin, origin).wait_recv()
        total = total + part_in[origin].astype(F32)
    moe_out[...] = total.astype(BF16)

    for k in range(1, tp_count):
        wz((t + k) % tp_count, t).wait_send()
    for dy, dx in around:
        peer = ep_peer(dy, dx)
        st(peer, e).wait_send()
        dx_copy(peer, e).wait_send()
        dp_copy(peer).wait_send()
        rt(peer, e).wait_send()
        for part in range(SPLIT):
            wx(part, peer, e).wait_send()
    for block in range(chips):
        pp(block).wait_send()
    for k in range(1, chips):
        zs((z + k) % chips, z).wait_send()
    for part in range(SPLIT):
        for origin in range(chips):
            line("pa", part, origin, 2 * z + 1 - core).wait_send()

            @pl.when((origin <= z) & (z + 1 < chips))
            def _():
                line("up", part, origin, t + 2).wait_send()

            @pl.when((origin >= z) & (z > 0))
            def _():
                line("dn", part, origin, t - 2).wait_send()


def local(
    queries,
    keys,
    values,
    out_gate,
    in_gate,
    forget_gate,
    out_gain,
    out_weight,
    moe_rows,
    moe_gain,
    routes,
    route_weight,
    expert_gate,
    expert_up,
    expert_down,
    shared_gate,
    shared_up,
    shared_down,
):
    tp_count = lax.axis_size("tp")
    ep_count = lax.axis_size("ep")
    count, depth = moe_rows.shape
    assert expert_gate.shape[0] == 1
    cap = 3 * count * routes.shape[1] // (2 * ep_count)
    slots = ep_count * cap
    heads = in_gate.shape[0]
    tok = queries.shape[0]
    held = heads * DK
    extra = -(-(1 + 2 * heads) // 8) * 8
    chips = tp_count // 2
    units, common = expert_gate.shape[2], shared_gate.shape[1]
    wide, features = out_weight.shape
    feat = features // tp_count
    share = wide // ep_count
    half = depth // 2
    side = 1
    while side * side < ep_count:
        side *= 2
    dma = pltpu.SemaphoreType.DMA

    def vm(*shape, dtype=BF16):
        return pltpu.VMEM(shape, dtype)

    scratch = [
        vm(ep_count, held + extra, 128, dtype=F32),
        vm(tok, heads * DV),
        vm(tp_count, tok, heads * DV),
        vm(tp_count, ep_count, share, feat),
        vm(count, depth),
        vm(2, ep_count, cap, half),
        vm(2, ep_count, cap, half),
        vm(depth, units),
        vm(depth, units),
        vm(units, depth),
        vm(depth, common),
        vm(depth, common),
        vm(common, depth),
        vm(slots, units),
        vm(count, common),
        vm(chips, slots + count, feat),
        vm(chips, slots + count, feat),
        vm(chips, ep_count, cap, feat),
        vm(chips, ep_count, cap, feat),
        vm(chips, count, feat, dtype=F32),
        vm(chips, count, feat),
        vm(chips, count, feat),
        vm(count, feat, dtype=F32),
        dma((7,)),
    ]
    scratch += [dma((tp_count,))] * 2
    scratch += [dma((SPLIT, ep_count))] * 2
    scratch += [dma((ep_count,))] * 6
    scratch += [dma((SPLIT, chips))] * 6
    scratch += [dma((chips,))] * 2
    scratch += [dma((ep_count,))] * 2
    scratch += [dma((chips,))] * 2
    return pl.pallas_call(
        functools.partial(step_kernel, ep_count, tp_count, side, cap),
        out_shape=(
            jax.ShapeDtypeStruct((tok, feat), BF16),
            jax.ShapeDtypeStruct((count, feat), BF16),
        ),
        in_specs=[VM] * 11 + [ANY] * 7,
        out_specs=(VM, VM),
        scratch_shapes=scratch,
        compiler_params=pltpu.CompilerParams(
            collective_id=0, has_side_effects=True, vmem_limit_bytes=60 * 1024 * 1024
        ),
        cost_estimate=pl.CostEstimate(
            flops=9_000_000_000, bytes_accessed=30_000_000, transcendentals=0
        ),
    )(
        queries,
        keys,
        values,
        out_gate,
        in_gate,
        forget_gate,
        out_gain.reshape(1, -1),
        moe_rows,
        moe_gain.reshape(1, -1),
        routes,
        route_weight,
        out_weight,
        expert_gate,
        expert_up,
        expert_down,
        shared_gate,
        shared_up,
        shared_down,
    )


def solution(mesh):
    return jax.shard_map(
        local,
        mesh=mesh,
        in_specs=(
            P("ep", "tp"),
            P("ep", "tp"),
            P("ep", "tp"),
            P("ep", "tp"),
            P("tp", "ep"),
            P("tp", "ep"),
            P("tp"),
            P("tp", None),
            P("ep", None),
            P(),
            P("ep", None),
            P("ep", None),
            P("ep", None, "tp"),
            P("ep", None, "tp"),
            P("ep", "tp", None),
            P(None, "tp"),
            P(None, "tp"),
            P("tp", None),
        ),
        out_specs=(P("ep", "tp"), P("ep", "tp")),
        check_vma=False,
    )
```

```python
import functools

import jax
import jax.numpy as jnp
from jax import lax
from jax.experimental import pallas as pl
from jax.experimental.pallas import tpu as pltpu
from jax.sharding import PartitionSpec as P

DK = 64
DV = 128
CH = 128
F32 = jnp.float32
BF16 = jnp.bfloat16
VM = pl.BlockSpec(memory_space=pltpu.VMEM)
ANY = pl.BlockSpec(memory_space=pl.ANY)
MESH = pl.DeviceIdType.MESH
SPLIT = 2


def gate_rows(ig, fg):
    lane = lax.broadcasted_iota(jnp.int32, ig.shape, 1)
    total = jnp.minimum(fg, 0.0) - jnp.log1p(jnp.exp(-jnp.abs(fg)))
    step = 1
    while step < CH:
        total = total + jnp.where(lane >= step, pltpu.roll(total, step, 1), 0.0)
        step *= 2
    level = ig - total
    top = level
    step = 1
    while step < CH:
        top = jnp.maximum(top, jnp.where(lane >= step, pltpu.roll(top, step, 1), -1e30))
        step *= 2
    return total, level, top


def columns_of(parts):
    rows = sum(part.shape[0] for part in parts)
    padded = -(-rows // 128) * 128
    if padded > rows:
        parts = list(parts) + [jnp.zeros((padded - rows, CH), F32)]
    return jnp.concatenate(parts, axis=0).T


def split_bf16(x):
    high = x.astype(BF16)
    return high, (x - high.astype(F32)).astype(BF16)


def weighted_keys(keys, cols, first, heads, chunks):
    lane_head = lax.broadcasted_iota(jnp.int32, keys.shape, 1) // DK
    weight = jnp.broadcast_to(cols[:, first : first + 1], keys.shape)
    for h in range(1, heads):
        at = first + h * chunks
        weight = jnp.where(lane_head == h, jnp.broadcast_to(cols[:, at : at + 1], keys.shape), weight)
    return split_bf16(keys.astype(F32) * weight)


def add_outer(kw, values):
    dims = (((0,), (0,)), ((), ()))
    return lax.dot_general(kw[0], values, dims, preferred_element_type=F32) + lax.dot_general(
        kw[1], values, dims, preferred_element_type=F32
    )


def pick_head(parts, shape, axis):
    head = lax.broadcasted_iota(jnp.int32, shape, axis) // DK
    out = jnp.broadcast_to(parts[0], shape)
    for h in range(1, len(parts)):
        out = jnp.where(head == h, jnp.broadcast_to(parts[h], shape), out)
    return out


def summary(heads, chunks, k_ref, v_ref, gates, out_ref, slot):
    width = heads * DK
    total, level, top = gates
    shape = total.shape
    chunk = lax.broadcasted_iota(jnp.int32, shape, 0) % chunks
    last = jnp.broadcast_to(total[:, CH - 1 : CH], shape)
    suffix = last
    step = 1
    while step < chunks:
        moved = pltpu.roll(suffix, shape[0] - step, 0)
        suffix = suffix + jnp.where(chunk + step < chunks, moved, 0.0)
        step *= 2
    reach = suffix + jnp.broadcast_to(top[:, CH - 1 : CH], shape)
    tops = [
        jnp.max(reach[h * chunks : (h + 1) * chunks], axis=0, keepdims=True) for h in range(heads)
    ]
    weight = [
        jnp.exp(
            level[h * chunks : (h + 1) * chunks] + suffix[h * chunks : (h + 1) * chunks] - tops[h]
        )
        for h in range(heads)
    ]
    cols = columns_of(weight)
    state = jnp.zeros((width, heads * DV + 128), F32)
    for c in range(chunks):
        rows = pl.ds(c * CH, CH)
        kw = weighted_keys(k_ref[rows, :], cols, c, heads, chunks)
        values = jnp.concatenate([v_ref[rows, :], jnp.ones((CH, 128), BF16)], axis=1)
        state = state + add_outer(kw, values)
    out_ref[slot] = jnp.zeros(out_ref.shape[1:], F32)
    out_ref[slot, 0:width, :] = pick_head(
        [state[:, h * DV : (h + 1) * DV] for h in range(heads)], (width, DV), 0
    )
    normal = state[:, heads * DV :].T
    out_ref[slot, width : width + 1, 0:width] = normal[0:1, :]
    for h in range(heads):
        out_ref[slot, width + 1 + h : width + 2 + h, :] = tops[h]
        at = width + 1 + heads + h
        out_ref[slot, at : at + 1, :] = suffix[h * chunks : h * chunks + 1]


def entering_state(heads, pos, sum_ref):
    width = heads * DK
    matrix = jnp.zeros((width, DV), F32)
    normal = jnp.zeros((1, width), F32)
    stab = [jnp.zeros((1, 128), F32) for _ in range(heads)]
    for e in range(sum_ref.shape[0]):
        reached = e < pos
        part = sum_ref.at[e]
        old_w, new_w, new_stab = [], [], []
        for h in range(heads):
            at = width + 1 + h
            carried = part[at + heads : at + heads + 1, :] + stab[h]
            there = part[at : at + 1, :]
            joined = jnp.maximum(carried, there)
            old_w.append(jnp.where(reached, jnp.exp(carried - joined), 1.0))
            new_w.append(jnp.where(reached, jnp.exp(there - joined), 0.0))
            new_stab.append(jnp.where(reached, joined, stab[h]))
        matrix = (
            pick_head(old_w, (width, DV), 0) * matrix
            + pick_head(new_w, (width, DV), 0) * part[0:width, :]
        )
        normal = (
            pick_head([w[:, 0:width] for w in old_w], (1, width), 1) * normal
            + pick_head([w[:, 0:width] for w in new_w], (1, width), 1)
            * part[width : width + 1, 0:width]
        )
        stab = new_stab
    normal_cols = jnp.broadcast_to(normal, (128, width)).T
    return jnp.concatenate([matrix] * heads + [normal_cols], axis=1), stab


def cell_blocks(
    heads, chunks, state, stab, gates, q_ref, k_ref, v_ref, og_ref, gain_ref, out_ref, after
):
    width = heads * DK
    total, level, top = gates
    shape = total.shape
    last = jnp.broadcast_to(total[:, CH - 1 : CH], shape)
    last_top = jnp.broadcast_to(top[:, CH - 1 : CH], shape)
    entering, leaving = [], []
    for h in range(heads):
        now = stab[h]
        for c in range(chunks):
            r = h * chunks + c
            entering.append(now)
            now = last[r : r + 1] + jnp.maximum(now, last_top[r : r + 1])
            leaving.append(now)
    entering = jnp.concatenate(entering, axis=0)
    leaving = jnp.concatenate(leaving, axis=0)
    peak = jnp.maximum(top, entering)
    decay = jnp.exp(last + entering - leaving)
    count = heads * chunks
    cols = columns_of(
        [
            peak,
            jnp.exp(entering - peak),
            jnp.exp(-(total + peak)),
            jnp.exp(last + level - leaving),
        ]
    )
    causal = lax.broadcasted_iota(jnp.int32, (CH, CH), 0) >= lax.broadcasted_iota(
        jnp.int32, (CH, CH), 1
    )
    lane_head = lax.broadcasted_iota(jnp.int32, (CH, width), 1) // DK
    for c in range(chunks):
        rows = pl.ds(c * CH, CH)
        keys = k_ref[rows, :]
        values = v_ref[rows, :]
        queries = q_ref[rows, :] * jnp.asarray(DK**-0.5, BF16)
        high, low = split_bf16(state)
        for h in range(heads):
            r = h * chunks + c
            mine = jnp.where(lane_head == h, queries, jnp.zeros_like(queries))
            raw = lax.dot_general(
                mine, keys, (((1,), (1,)), ((), ())), preferred_element_type=F32
            )
            logs = level[r : r + 1, :] - cols[:, r : r + 1]
            scores = raw * jnp.exp(jnp.where(causal, logs, -jnp.inf))
            inner = jnp.dot(
                scores.astype(BF16), values[:, h * DV : (h + 1) * DV], preferred_element_type=F32
            )
            across = 0.0
            for piece in (high, low):
                rhs = jnp.concatenate(
                    [piece[:, h * DV : (h + 1) * DV], piece[:, heads * DV :]], axis=1
                )
                across = across + jnp.dot(mine, rhs, preferred_element_type=F32)
            inter = cols[:, count + r : count + r + 1]
            signed = jnp.sum(scores, axis=1, keepdims=True) + inter * across[:, DV : DV + 1]
            divisor = jnp.maximum(jnp.abs(signed), cols[:, 2 * count + r : 2 * count + r + 1])
            cells = (inner + inter * across[:, :DV]) * (1.0 / divisor)
            at = slice(h * DV, (h + 1) * DV)
            gate = og_ref[rows, at].astype(F32)
            out_ref[rows, at] = (cells / (1.0 + jnp.exp(-gate)) * gain_ref[:, at]).astype(BF16)
        if c + 1 < chunks:
            kw = weighted_keys(keys, cols, 3 * count + c, heads, chunks)
            scale = pick_head(
                [decay[h * chunks + c : h * chunks + c + 1] for h in range(heads)], (width, 128), 0
            )
            rhs = jnp.concatenate([values, jnp.ones((CH, 128), BF16)], axis=1)
            state = state * jnp.concatenate([scale] * (heads + 1), axis=1) + add_outer(kw, rhs)
        after(c)


def tiles(width, most):
    return min(width, most)


def step_kernel(
    ep_count,
    tp_count,
    side,
    cap,
    ig_ref,
    fg_ref,
    gain_ref,
    mg_ref,
    routes_ref,
    rw_ref,
    q_hbm,
    k_hbm,
    v_hbm,
    og_hbm,
    rows_hbm,
    ow_hbm,
    eg_hbm,
    eu_hbm,
    ed_hbm,
    sg_hbm,
    su_hbm,
    sd_hbm,
    mixer_out,
    moe_out,
    sums,
    own,
    mixed,
    wcols,
    out_rows,
    tokens,
    q_ref,
    k_ref,
    v_ref,
    og_ref,
    normed,
    staged,
    arrived,
    eg,
    eu,
    ed,
    sg,
    su,
    sd,
    hidden,
    shared_hidden,
    give,
    take,
    reduced,
    returned,
    shared_own,
    part_out,
    part_in,
    final,
    load_sem,
    out_sem,
    wz_s,
    wz_r,
    wx_s,
    wx_r,
    wf_s,
    st_s,
    st_r,
    dx_s,
    dx_r,
    dp_s,
    dp_r,
    up_s,
    up_r,
    dn_s,
    dn_r,
    pa_s,
    pa_r,
    pp_s,
    pp_r,
    rt_s,
    rt_r,
    zs_s,
    zs_r,
):
    e, t = lax.axis_index("ep"), lax.axis_index("tp")
    z, core = t // 2, t % 2
    chips = tp_count // 2
    heads = ig_ref.shape[0]
    tok = q_ref.shape[0]
    chunks = tok // CH
    count, depth = tokens.shape
    half = depth // 2
    feat = mixer_out.shape[1]
    share = wcols.shape[2]
    slots = ep_count * cap
    group = tp_count // SPLIT
    batch = chips // SPLIT
    seg = tok // SPLIT

    def ep_peer(dy, dx):
        deep = ep_count // side
        return ((e // side + dy) % deep) * side + (e % side + dx) % side

    around = [(dy, dx) for dy in range(ep_count // side) for dx in range(side)][1:]
    around = around[::-1]

    def remote(src, dst, send, recv, where):
        return pltpu.make_async_remote_copy(
            src_ref=src, dst_ref=dst, send_sem=send, recv_sem=recv, device_id=where,
            device_id_type=MESH,
        )

    barrier = pltpu.get_barrier_semaphore()
    for dy, dx in around:
        pl.semaphore_signal(barrier, inc=1, device_id=(ep_peer(dy, dx), t), device_id_type=MESH)
    for k in range(1, tp_count):
        pl.semaphore_signal(
            barrier, inc=1, device_id=(e, (t + k) % tp_count), device_id_type=MESH
        )
    loads = {}
    for name, src, dst in (
        ("k", k_hbm, k_ref),
        ("v", v_hbm, v_ref),
        ("tokens", rows_hbm, tokens),
        ("sg", sg_hbm, sg),
        ("su", su_hbm, su),
        ("q", q_hbm, q_ref),
        ("og", og_hbm, og_ref),
        (
            "own",
            ow_hbm.at[
                pl.ds(pl.multiple_of(e * share, share), share),
                pl.ds(pl.multiple_of(t * feat, feat), feat),
            ],
            wcols.at[t, e],
        ),
        ("eg", eg_hbm.at[0], eg),
        ("eu", eu_hbm.at[0], eu),
        ("ed", ed_hbm.at[0], ed),
        ("sd", sd_hbm, sd),
    ):
        loads[name] = pltpu.make_async_copy(src, dst, load_sem.at[len(loads)])
        loads[name].start()
    pl.semaphore_wait(barrier, ep_count - 1 + tp_count - 1)

    def wz(to, origin):
        return remote(
            ow_hbm.at[
                pl.ds(pl.multiple_of(e * share, share), share),
                pl.ds(pl.multiple_of(to * feat, feat), feat),
            ],
            wcols.at[origin, e],
            wz_s.at[to],
            wz_r.at[origin],
            (e, to),
        )

    for k in range(1, tp_count):
        wz((t + k) % tp_count, t).start()

    def stacked(ref):
        return jnp.concatenate(
            [ref[h : h + 1, c * CH : (c + 1) * CH] for h in range(heads) for c in range(chunks)],
            axis=0,
        )

    gates = gate_rows(stacked(ig_ref), stacked(fg_ref))
    loads["k"].wait()
    loads["v"].wait()
    summary(heads, chunks, k_ref, v_ref, gates, sums, e)

    def st(peer, origin):
        return remote(
            sums.at[origin], sums.at[origin], st_s.at[peer], st_r.at[origin], (peer, t)
        )

    for dy, dx in around:
        st(ep_peer(dy, dx), e).start()

    loads["tokens"].wait()
    width = tiles(half, 512)
    square = jnp.zeros((count, 1), F32)
    for n in range(0, depth, width):
        wide = tokens[:, n : n + width].astype(F32)
        square = square + jnp.sum(wide * wide, axis=1, keepdims=True)
    inverse = lax.rsqrt(square / depth + 1e-06)
    for n in range(0, depth, width):
        wide = tokens[:, n : n + width].astype(F32)
        normed[:, n : n + width] = (wide * inverse * mg_ref[:, n : n + width]).astype(BF16)

    topk = routes_ref.shape[0]
    table = columns_of([routes_ref[...].astype(F32), rw_ref[...]])
    lane = lax.broadcasted_iota(jnp.int32, (count, 128), 1).astype(F32)
    named = [lane == table[:, k : k + 1] for k in range(topk)]
    member = named[0]
    for k in range(1, topk):
        member = member | named[k]
    earlier = lax.broadcasted_iota(jnp.int32, (count, count), 0) > lax.broadcasted_iota(
        jnp.int32, (count, count), 1
    )
    before = jnp.dot(
        jnp.where(earlier, 1.0, 0.0).astype(BF16),
        jnp.where(member, 1.0, 0.0).astype(BF16),
        preferred_element_type=F32,
    )
    slot_no = lax.broadcasted_iota(jnp.int32, (count, slots), 1).astype(F32)
    place = jnp.zeros((count, slots), F32)
    weight = jnp.zeros((count, slots), F32)
    for k in range(topk):
        ahead = jnp.sum(jnp.where(named[k], before, 0.0), axis=1, keepdims=True)
        hit = slot_no == table[:, k : k + 1] * cap + ahead
        place = jnp.where(hit, 1.0, place)
        weight = jnp.where(hit, table[:, topk + k : topk + k + 1], weight)
    place = place.astype(BF16)
    weight_high, weight_low = split_bf16(weight)

    def stage(side_no):
        for n in range(0, half, width):
            cols = pl.ds(pl.multiple_of(side_no * half + n, width), width)
            moved = lax.dot_general(
                place, normed[:, cols], (((0,), (0,)), ((), ())), preferred_element_type=F32
            ).astype(BF16)
            for x in range(ep_count):
                staged[side_no, x, :, n : n + width] = moved[x * cap : (x + 1) * cap]

    def dx_copy(peer, origin):
        return remote(
            staged.at[core, peer],
            arrived.at[core, origin],
            dx_s.at[peer],
            dx_r.at[origin],
            (peer, t),
        )

    def dp_copy(origin):
        return remote(
            arrived.at[core, origin],
            arrived.at[core, origin],
            dp_s.at[origin],
            dp_r.at[origin],
            (e, 2 * z + 1 - core),
        )

    def dp_other(origin):
        return remote(
            arrived.at[core, origin],
            arrived.at[1 - core, origin],
            dp_s.at[origin],
            dp_r.at[origin],
            (e, 2 * z + 1 - core),
        )

    stage(core)
    stage(1 - core)
    for s in range(2):
        arrived[s, e] = staged[s, e]

    loads["sg"].wait()
    loads["su"].wait()
    gate = jnp.dot(normed[...], sg[...], preferred_element_type=F32)
    up = jnp.dot(normed[...], su[...], preferred_element_type=F32)
    shared_hidden[...] = (gate / (1.0 + jnp.exp(-gate)) * up).astype(BF16)

    def line(kind, part, origin, where):
        sems = {"up": (up_s, up_r), "dn": (dn_s, dn_r), "pa": (pa_s, pa_r)}[kind]
        ref = mixed.at[2 * origin + core, pl.ds(part * seg, seg)]
        return remote(
            ref, ref, sems[0].at[part, origin], sems[1].at[part, origin], (e, where)
        )

    def line_other(part, origin):
        ref = mixed.at[2 * origin + 1 - core, pl.ds(part * seg, seg)]
        return remote(
            ref, ref, pa_s.at[part, origin], pa_r.at[part, origin], (e, 2 * z + 1 - core)
        )

    def go_up(part, origin):
        @pl.when(z + 1 < chips)
        def _():
            line("up", part, origin, t + 2).start()

    def go_down(part, origin):
        @pl.when(z > 0)
        def _():
            line("dn", part, origin, t - 2).start()

    def go_across(part, origin):
        line("pa", part, origin, 2 * z + 1 - core).start()

    def after(c):
        if (c + 1) % (chunks // SPLIT) == 0:
            part = (c + 1) // (chunks // SPLIT) - 1
            mixed[t, part * seg : (part + 1) * seg] = own[part * seg : (part + 1) * seg]
            go_up(part, z)
            go_down(part, z)
            go_across(part, z)

    def relay(step, part):
        if step >= chips:
            return

        @pl.when(z >= step)
        def _():
            line("up", part, z - step, t - 2).wait_recv()
            go_up(part, z - step)
            go_across(part, z - step)

        @pl.when(z + step < chips)
        def _():
            line("dn", part, z + step, t + 2).wait_recv()
            go_down(part, z + step)
            go_across(part, z + step)

    for dy, dx in around:
        peer = ep_peer(dy, dx)
        st(peer, peer).wait_recv()
    for dy, dx in around:
        dx_copy(ep_peer(dy, dx), e).start()
    loads["q"].wait()
    loads["og"].wait()
    state, stab = entering_state(heads, e, sums)
    cell_blocks(
        heads, chunks, state, stab, gates, q_ref, k_ref, v_ref, og_ref, gain_ref, own, after
    )

    rowwise = [(dy, dx) for dy, dx in around if dy == 0]
    columnwise = [(dy, dx) for dy, dx in around if dx == 0]

    def wx(part, peer, origin):
        ref = wcols.at[pl.ds(part * group, group), origin]
        return remote(ref, ref, wx_s.at[part, peer], wx_r.at[part, origin], (peer, t))

    def wf(part, peer, origin):
        ref = wcols.at[pl.ds(part * group, group), origin]
        return remote(ref, ref, wf_s.at[origin, peer], wx_r.at[part, origin], (peer, t))

    paths = ((rowwise, columnwise), (columnwise, rowwise))

    relay(1, 0)
    for dy, dx in around:
        origin = ep_peer(dy, dx)
        dx_copy(origin, origin).wait_recv()
        dp_copy(origin).start()
    loads["own"].wait()
    for k in range(1, tp_count):
        wz((t + k) % tp_count, (t + k) % tp_count).wait_recv()
    for part in range(SPLIT):
        for dy, dx in rowwise + columnwise:
            wx(part, ep_peer(dy, dx), e).start()
    relay(1, 1)
    for dy, dx in around:
        dp_other(ep_peer(dy, dx)).wait_recv()

    loads["eg"].wait()
    loads["eu"].wait()
    units = eg.shape[1]
    tile = tiles(units, 256)

    def both(weights, n):
        return sum(
            jnp.dot(
                arrived[s].reshape(slots, half),
                weights[s * half : (s + 1) * half, n : n + tile],
                preferred_element_type=F32,
            )
            for s in range(2)
        )

    for n in range(0, units, tile):
        gate = both(eg, n)
        up = both(eu, n)
        hidden[:, n : n + tile] = (gate / (1.0 + jnp.exp(-gate)) * up).astype(BF16)

    loads["ed"].wait()
    loads["sd"].wait()

    def pp(block):
        return remote(
            give.at[block], take.at[block], pp_s.at[block], pp_r.at[block],
            (e, 2 * z + 1 - core),
        )

    def products(block, owner):
        cols = pl.ds(pl.multiple_of((2 * block + owner) * feat, feat), feat)
        return (
            jnp.dot(hidden[...], ed[:, cols], preferred_element_type=F32),
            jnp.dot(shared_hidden[...], sd[:, cols], preferred_element_type=F32),
        )

    for block in range(chips):
        routed, common = products(block, 1 - core)
        give[block, 0:slots] = routed.astype(BF16)
        give[block, slots:] = common.astype(BF16)
        pp(block).start()
    relay(2, 0)

    def rt(part, peer, origin):
        blocks = pl.ds(part * batch, batch)
        return remote(
            reduced.at[blocks, peer],
            returned.at[blocks, origin],
            rt_s.at[part, peer],
            rt_r.at[part, origin],
            (peer, t),
        )

    for block in range(chips):
        routed, common = products(block, core)
        pp(block).wait_recv()
        total = (routed + take[block, 0:slots].astype(F32)).astype(BF16)
        for x in range(ep_count):
            reduced[block, x] = total[x * cap : (x + 1) * cap]
        shared_own[block] = common + take[block, slots:].astype(F32)
        if (block + 1) % batch == 0:
            for dy, dx in around:
                rt(block // batch, ep_peer(dy, dx), e).start()
    for block in range(chips):
        returned[block, e] = reduced[block, e]
    relay(2, 1)
    for part, (near, far) in enumerate(paths):
        for dy, dx in near:
            origin = ep_peer(dy, dx)
            wx(part, origin, origin).wait_recv()
            for fy, fx in far:
                wf(part, ep_peer(fy, fx), origin).start()

    def zs(to, origin):
        return remote(
            part_out.at[to], part_in.at[origin], zs_s.at[to], zs_r.at[origin], (e, 2 * to + core)
        )

    for part in range(SPLIT):
        for dy, dx in around:
            origin = ep_peer(dy, dx)
            rt(part, origin, origin).wait_recv()
        for block in range(part * batch, (part + 1) * batch):
            results = returned[block].reshape(slots, feat)
            total = (
                jnp.dot(weight_high, results, preferred_element_type=F32)
                + jnp.dot(weight_low, results, preferred_element_type=F32)
                + shared_own[block]
            )
            part_out[block] = total.astype(BF16)

            @pl.when(z == block)
            def _():
                final[...] = total

            @pl.when(z != block)
            def _():
                zs(block, z).start()

        for step in range(3, chips):
            relay(step, part)

    for dy, dx in around:
        origin = ep_peer(dy, dx)
        if dy == 0:
            wx(1, origin, origin).wait_recv()
        elif dx == 0:
            wx(0, origin, origin).wait_recv()
        else:
            for part in range(SPLIT):
                wx(part, origin, origin).wait_recv()
    for part in range(SPLIT):
        for origin in range(chips):
            line_other(part, origin).wait_recv()
    step_rows = tiles(tok, 256)

    @pl.loop(0, tok // step_rows)
    def _(i):
        rows = pl.ds(pl.multiple_of(i * step_rows, step_rows), step_rows)
        total = 0.0
        for b in range(tp_count):
            total = total + jnp.dot(
                mixed[b, rows],
                wcols[b].reshape(ep_count * share, feat),
                preferred_element_type=F32,
            )
        out_rows[rows] = total.astype(BF16)
        pltpu.make_async_copy(out_rows.at[rows], mixer_out.at[rows], out_sem.at[i]).start()

    total = final[...]
    for k in range(1, chips):
        origin = (z + k) % chips
        zs(origin, origin).wait_recv()
        total = total + part_in[origin].astype(F32)
    moe_out[...] = total.astype(BF16)

    for k in range(1, tp_count):
        wz((t + k) % tp_count, t).wait_send()
    for dy, dx in rowwise + columnwise:
        for part in range(SPLIT):
            wx(part, ep_peer(dy, dx), e).wait_send()
    for part, (near, far) in enumerate(paths):
        for dy, dx in near:
            for fy, fx in far:
                wf(part, ep_peer(fy, fx), ep_peer(dy, dx)).wait_send()
    for dy, dx in around:
        peer = ep_peer(dy, dx)
        st(peer, e).wait_send()
        dx_copy(peer, e).wait_send()
        dp_copy(peer).wait_send()
        for part in range(SPLIT):
            rt(part, peer, e).wait_send()
    for block in range(chips):
        pp(block).wait_send()
    for block in range(chips):

        @pl.when(z != block)
        def _():
            zs(block, z).wait_send()

    for part in range(SPLIT):
        for origin in range(chips):
            line("pa", part, origin, 2 * z + 1 - core).wait_send()

            @pl.when((origin <= z) & (z + 1 < chips))
            def _():
                line("up", part, origin, t + 2).wait_send()

            @pl.when((origin >= z) & (z > 0))
            def _():
                line("dn", part, origin, t - 2).wait_send()

    @pl.loop(0, tok // step_rows)
    def _(i):
        rows = pl.ds(pl.multiple_of(i * step_rows, step_rows), step_rows)
        pltpu.make_async_copy(out_rows.at[rows], mixer_out.at[rows], out_sem.at[i]).wait()


def local(
    queries,
    keys,
    values,
    out_gate,
    in_gate,
    forget_gate,
    out_gain,
    out_weight,
    moe_rows,
    moe_gain,
    routes,
    route_weight,
    expert_gate,
    expert_up,
    expert_down,
    shared_gate,
    shared_up,
    shared_down,
):
    tp_count = lax.axis_size("tp")
    ep_count = lax.axis_size("ep")
    count, depth = moe_rows.shape
    assert expert_gate.shape[0] == 1
    cap = 3 * count * routes.shape[1] // (2 * ep_count)
    slots = ep_count * cap
    heads = in_gate.shape[0]
    tok = queries.shape[0]
    held = heads * DK
    extra = -(-(1 + 2 * heads) // 8) * 8
    chips = tp_count // 2
    units, common = expert_gate.shape[2], shared_gate.shape[1]
    wide, features = out_weight.shape
    feat = features // tp_count
    share = wide // ep_count
    half = depth // 2
    side = 1
    while side * side < ep_count:
        side *= 2
    dma = pltpu.SemaphoreType.DMA

    def vm(*shape, dtype=BF16):
        return pltpu.VMEM(shape, dtype)

    scratch = [
        vm(ep_count, held + extra, 128, dtype=F32),
        vm(tok, heads * DV),
        vm(tp_count, tok, heads * DV),
        vm(tp_count, ep_count, share, feat),
        vm(tok, feat),
        vm(count, depth),
        vm(tok, held),
        vm(tok, held),
        vm(tok, heads * DV),
        vm(tok, heads * DV),
        vm(count, depth),
        vm(2, ep_count, cap, half),
        vm(2, ep_count, cap, half),
        vm(depth, units),
        vm(depth, units),
        vm(units, depth),
        vm(depth, common),
        vm(depth, common),
        vm(common, depth),
        vm(slots, units),
        vm(count, common),
        vm(chips, slots + count, feat),
        vm(chips, slots + count, feat),
        vm(chips, ep_count, cap, feat),
        vm(chips, ep_count, cap, feat),
        vm(chips, count, feat, dtype=F32),
        vm(chips, count, feat),
        vm(chips, count, feat),
        vm(count, feat, dtype=F32),
        dma((12,)),
        dma((-(-tok // 256),)),
    ]
    scratch += [dma((tp_count,))] * 2
    scratch += [dma((SPLIT, ep_count))] * 2
    scratch += [dma((ep_count, ep_count))]
    scratch += [dma((ep_count,))] * 6
    scratch += [dma((SPLIT, chips))] * 6
    scratch += [dma((chips,))] * 2
    scratch += [dma((SPLIT, ep_count))] * 2
    scratch += [dma((chips,))] * 2
    return pl.pallas_call(
        functools.partial(step_kernel, ep_count, tp_count, side, cap),
        out_shape=(
            jax.ShapeDtypeStruct((tok, feat), BF16),
            jax.ShapeDtypeStruct((count, feat), BF16),
        ),
        in_specs=[VM] * 6 + [ANY] * 12,
        out_specs=(ANY, VM),
        scratch_shapes=scratch,
        compiler_params=pltpu.CompilerParams(
            collective_id=0, has_side_effects=True, vmem_limit_bytes=60 * 1024 * 1024
        ),
        cost_estimate=pl.CostEstimate(
            flops=9_000_000_000, bytes_accessed=30_000_000, transcendentals=0
        ),
    )(
        in_gate,
        forget_gate,
        out_gain.reshape(1, -1),
        moe_gain.reshape(1, -1),
        routes.T,
        route_weight.T,
        queries,
        keys,
        values,
        out_gate,
        moe_rows,
        out_weight,
        expert_gate,
        expert_up,
        expert_down,
        shared_gate,
        shared_up,
        shared_down,
    )


def solution(mesh):
    return jax.shard_map(
        local,
        mesh=mesh,
        in_specs=(
            P("ep", "tp"),
            P("ep", "tp"),
            P("ep", "tp"),
            P("ep", "tp"),
            P("tp", "ep"),
            P("tp", "ep"),
            P("tp"),
            P("tp", None),
            P("ep", None),
            P(),
            P("ep", None),
            P("ep", None),
            P("ep", None, "tp"),
            P("ep", None, "tp"),
            P("ep", "tp", None),
            P(None, "tp"),
            P(None, "tp"),
            P("tp", None),
        ),
        out_specs=(P("ep", "tp"), P("ep", "tp")),
        check_vma=False,
    )
```

```python
import functools

import jax
import jax.numpy as jnp
from jax import lax
from jax.experimental import pallas as pl
from jax.experimental.pallas import tpu as pltpu
from jax.sharding import PartitionSpec as P

DK = 64
DV = 128
CH = 128
F32 = jnp.float32
BF16 = jnp.bfloat16
VM = pl.BlockSpec(memory_space=pltpu.VMEM)
ANY = pl.BlockSpec(memory_space=pl.ANY)
MESH = pl.DeviceIdType.MESH
SPLIT = 2


def gate_rows(ig, fg):
    lane = lax.broadcasted_iota(jnp.int32, ig.shape, 1)
    total = jnp.minimum(fg, 0.0) - jnp.log1p(jnp.exp(-jnp.abs(fg)))
    step = 1
    while step < CH:
        total = total + jnp.where(lane >= step, pltpu.roll(total, step, 1), 0.0)
        step *= 2
    level = ig - total
    top = level
    step = 1
    while step < CH:
        top = jnp.maximum(top, jnp.where(lane >= step, pltpu.roll(top, step, 1), -1e30))
        step *= 2
    return total, level, top


def columns_of(parts):
    rows = sum(part.shape[0] for part in parts)
    padded = -(-rows // 128) * 128
    if padded > rows:
        parts = list(parts) + [jnp.zeros((padded - rows, CH), F32)]
    return jnp.concatenate(parts, axis=0).T


def split_bf16(x):
    high = x.astype(BF16)
    return high, (x - high.astype(F32)).astype(BF16)


def weighted_keys(keys, cols, first, heads, chunks):
    lane_head = lax.broadcasted_iota(jnp.int32, keys.shape, 1) // DK
    weight = jnp.broadcast_to(cols[:, first : first + 1], keys.shape)
    for h in range(1, heads):
        at = first + h * chunks
        weight = jnp.where(lane_head == h, jnp.broadcast_to(cols[:, at : at + 1], keys.shape), weight)
    return split_bf16(keys.astype(F32) * weight)


def add_outer(kw, values):
    dims = (((0,), (0,)), ((), ()))
    return lax.dot_general(kw[0], values, dims, preferred_element_type=F32) + lax.dot_general(
        kw[1], values, dims, preferred_element_type=F32
    )


def pick_head(parts, shape, axis):
    head = lax.broadcasted_iota(jnp.int32, shape, axis) // DK
    out = jnp.broadcast_to(parts[0], shape)
    for h in range(1, len(parts)):
        out = jnp.where(head == h, jnp.broadcast_to(parts[h], shape), out)
    return out


def summary(heads, chunks, k_ref, v_ref, gates, out_ref, slot):
    width = heads * DK
    total, level, top = gates
    shape = total.shape
    chunk = lax.broadcasted_iota(jnp.int32, shape, 0) % chunks
    last = jnp.broadcast_to(total[:, CH - 1 : CH], shape)
    suffix = last
    step = 1
    while step < chunks:
        moved = pltpu.roll(suffix, shape[0] - step, 0)
        suffix = suffix + jnp.where(chunk + step < chunks, moved, 0.0)
        step *= 2
    reach = suffix + jnp.broadcast_to(top[:, CH - 1 : CH], shape)
    tops = [
        jnp.max(reach[h * chunks : (h + 1) * chunks], axis=0, keepdims=True) for h in range(heads)
    ]
    weight = [
        jnp.exp(
            level[h * chunks : (h + 1) * chunks] + suffix[h * chunks : (h + 1) * chunks] - tops[h]
        )
        for h in range(heads)
    ]
    cols = columns_of(weight)
    state = jnp.zeros((width, heads * DV + 128), F32)
    for c in range(chunks):
        rows = pl.ds(c * CH, CH)
        kw = weighted_keys(k_ref[rows, :], cols, c, heads, chunks)
        values = jnp.concatenate([v_ref[rows, :], jnp.ones((CH, 128), BF16)], axis=1)
        state = state + add_outer(kw, values)
    out_ref[slot] = jnp.zeros(out_ref.shape[1:], F32)
    out_ref[slot, 0:width, :] = pick_head(
        [state[:, h * DV : (h + 1) * DV] for h in range(heads)], (width, DV), 0
    )
    normal = state[:, heads * DV :].T
    out_ref[slot, width : width + 1, 0:width] = normal[0:1, :]
    for h in range(heads):
        out_ref[slot, width + 1 + h : width + 2 + h, :] = tops[h]
        at = width + 1 + heads + h
        out_ref[slot, at : at + 1, :] = suffix[h * chunks : h * chunks + 1]


def entering_state(heads, pos, sum_ref):
    width = heads * DK
    matrix = jnp.zeros((width, DV), F32)
    normal = jnp.zeros((1, width), F32)
    stab = [jnp.zeros((1, 128), F32) for _ in range(heads)]
    for e in range(sum_ref.shape[0]):
        reached = e < pos
        part = sum_ref.at[e]
        old_w, new_w, new_stab = [], [], []
        for h in range(heads):
            at = width + 1 + h
            carried = part[at + heads : at + heads + 1, :] + stab[h]
            there = part[at : at + 1, :]
            joined = jnp.maximum(carried, there)
            old_w.append(jnp.where(reached, jnp.exp(carried - joined), 1.0))
            new_w.append(jnp.where(reached, jnp.exp(there - joined), 0.0))
            new_stab.append(jnp.where(reached, joined, stab[h]))
        matrix = (
            pick_head(old_w, (width, DV), 0) * matrix
            + pick_head(new_w, (width, DV), 0) * part[0:width, :]
        )
        normal = (
            pick_head([w[:, 0:width] for w in old_w], (1, width), 1) * normal
            + pick_head([w[:, 0:width] for w in new_w], (1, width), 1)
            * part[width : width + 1, 0:width]
        )
        stab = new_stab
    normal_cols = jnp.broadcast_to(normal, (128, width)).T
    return jnp.concatenate([matrix] * heads + [normal_cols], axis=1), stab


def cell_blocks(
    heads, chunks, state, stab, gates, q_ref, k_ref, v_ref, og_ref, gain_ref, out_ref, after
):
    width = heads * DK
    total, level, top = gates
    shape = total.shape
    last = jnp.broadcast_to(total[:, CH - 1 : CH], shape)
    last_top = jnp.broadcast_to(top[:, CH - 1 : CH], shape)
    entering, leaving = [], []
    for h in range(heads):
        now = stab[h]
        for c in range(chunks):
            r = h * chunks + c
            entering.append(now)
            now = last[r : r + 1] + jnp.maximum(now, last_top[r : r + 1])
            leaving.append(now)
    entering = jnp.concatenate(entering, axis=0)
    leaving = jnp.concatenate(leaving, axis=0)
    peak = jnp.maximum(top, entering)
    decay = jnp.exp(last + entering - leaving)
    count = heads * chunks
    cols = columns_of(
        [
            peak,
            jnp.exp(entering - peak),
            jnp.exp(-(total + peak)),
            jnp.exp(last + level - leaving),
        ]
    )
    causal = lax.broadcasted_iota(jnp.int32, (CH, CH), 0) >= lax.broadcasted_iota(
        jnp.int32, (CH, CH), 1
    )
    lane_head = lax.broadcasted_iota(jnp.int32, (CH, width), 1) // DK
    for c in range(chunks):
        rows = pl.ds(c * CH, CH)
        keys = k_ref[rows, :]
        values = v_ref[rows, :]
        queries = q_ref[rows, :] * jnp.asarray(DK**-0.5, BF16)
        high, low = split_bf16(state)
        for h in range(heads):
            r = h * chunks + c
            mine = jnp.where(lane_head == h, queries, jnp.zeros_like(queries))
            raw = lax.dot_general(
                mine, keys, (((1,), (1,)), ((), ())), preferred_element_type=F32
            )
            logs = level[r : r + 1, :] - cols[:, r : r + 1]
            scores = raw * jnp.exp(jnp.where(causal, logs, -jnp.inf))
            inner = jnp.dot(
                scores.astype(BF16), values[:, h * DV : (h + 1) * DV], preferred_element_type=F32
            )
            across = 0.0
            for piece in (high, low):
                rhs = jnp.concatenate(
                    [piece[:, h * DV : (h + 1) * DV], piece[:, heads * DV :]], axis=1
                )
                across = across + jnp.dot(mine, rhs, preferred_element_type=F32)
            inter = cols[:, count + r : count + r + 1]
            signed = jnp.sum(scores, axis=1, keepdims=True) + inter * across[:, DV : DV + 1]
            divisor = jnp.maximum(jnp.abs(signed), cols[:, 2 * count + r : 2 * count + r + 1])
            cells = (inner + inter * across[:, :DV]) * (1.0 / divisor)
            at = slice(h * DV, (h + 1) * DV)
            gate = og_ref[rows, at].astype(F32)
            out_ref[rows, at] = (cells / (1.0 + jnp.exp(-gate)) * gain_ref[:, at]).astype(BF16)
        if c + 1 < chunks:
            kw = weighted_keys(keys, cols, 3 * count + c, heads, chunks)
            scale = pick_head(
                [decay[h * chunks + c : h * chunks + c + 1] for h in range(heads)], (width, 128), 0
            )
            rhs = jnp.concatenate([values, jnp.ones((CH, 128), BF16)], axis=1)
            state = state * jnp.concatenate([scale] * (heads + 1), axis=1) + add_outer(kw, rhs)
        after(c)


def tiles(width, most):
    return min(width, most)


def step_kernel(
    ep_count,
    tp_count,
    side,
    cap,
    ig_ref,
    fg_ref,
    gain_ref,
    mg_ref,
    routes_ref,
    rw_ref,
    q_hbm,
    k_hbm,
    v_hbm,
    og_hbm,
    rows_hbm,
    ow_hbm,
    eg_hbm,
    eu_hbm,
    ed_hbm,
    sg_hbm,
    su_hbm,
    sd_hbm,
    mixer_out,
    moe_out,
    sums,
    own,
    mixed,
    wcols,
    out_rows,
    tokens,
    q_ref,
    k_ref,
    v_ref,
    og_ref,
    normed,
    staged,
    arrived,
    eg,
    eu,
    ed,
    sg,
    su,
    sd,
    hidden,
    shared_hidden,
    give,
    take,
    reduced,
    returned,
    shared_own,
    part_out,
    part_in,
    final,
    own_rows,
    load_sem,
    out_sem,
    wz_s,
    wz_r,
    wx_s,
    wx_r,
    wf_s,
    st_s,
    st_r,
    dx_s,
    dx_r,
    dp_s,
    dp_r,
    up_s,
    up_r,
    dn_s,
    dn_r,
    pa_s,
    pa_r,
    pp_s,
    pp_r,
    rt_s,
    rt_r,
    zs_s,
    zs_r,
):
    e, t = lax.axis_index("ep"), lax.axis_index("tp")
    z, core = t // 2, t % 2
    chips = tp_count // 2
    heads = ig_ref.shape[0]
    tok = q_ref.shape[0]
    chunks = tok // CH
    count, depth = tokens.shape
    half = depth // 2
    feat = mixer_out.shape[1]
    share = wcols.shape[2]
    slots = ep_count * cap
    group = tp_count // SPLIT
    batch = chips // SPLIT
    order = [b for i in range(chips // 2) for b in (i, chips - 1 - i)]
    seg = tok // SPLIT

    def ep_peer(dy, dx):
        deep = ep_count // side
        return ((e // side + dy) % deep) * side + (e % side + dx) % side

    around = [(dy, dx) for dy in range(ep_count // side) for dx in range(side)][1:]
    around = around[::-1]

    def remote(src, dst, send, recv, where):
        return pltpu.make_async_remote_copy(
            src_ref=src, dst_ref=dst, send_sem=send, recv_sem=recv, device_id=where,
            device_id_type=MESH,
        )

    barrier = pltpu.get_barrier_semaphore()
    for dy, dx in around:
        pl.semaphore_signal(barrier, inc=1, device_id=(ep_peer(dy, dx), t), device_id_type=MESH)
    for k in range(1, tp_count):
        pl.semaphore_signal(
            barrier, inc=1, device_id=(e, (t + k) % tp_count), device_id_type=MESH
        )
    loads = {}
    for name, src, dst in (
        ("tokens", rows_hbm, tokens),
        ("k", k_hbm, k_ref),
        ("v", v_hbm, v_ref),
        ("sg", sg_hbm, sg),
        ("su", su_hbm, su),
        ("q", q_hbm, q_ref),
        ("og", og_hbm, og_ref),
        (
            "own",
            ow_hbm.at[
                pl.ds(pl.multiple_of(e * share, share), share),
                pl.ds(pl.multiple_of(t * feat, feat), feat),
            ],
            wcols.at[t, e],
        ),
        ("eg", eg_hbm.at[0], eg),
        ("eu", eu_hbm.at[0], eu),
        ("ed", ed_hbm.at[0], ed),
        ("sd", sd_hbm, sd),
    ):
        loads[name] = pltpu.make_async_copy(src, dst, load_sem.at[len(loads)])
        loads[name].start()
    pl.semaphore_wait(barrier, ep_count - 1 + tp_count - 1)

    def wz(to, origin):
        return remote(
            ow_hbm.at[
                pl.ds(pl.multiple_of(e * share, share), share),
                pl.ds(pl.multiple_of(to * feat, feat), feat),
            ],
            wcols.at[origin, e],
            wz_s.at[to],
            wz_r.at[origin],
            (e, to),
        )

    for k in range(1, tp_count):
        wz((t + k) % tp_count, t).start()

    loads["tokens"].wait()
    width = tiles(half, 512)
    square = jnp.zeros((count, 1), F32)
    for n in range(0, depth, width):
        wide = tokens[:, n : n + width].astype(F32)
        square = square + jnp.sum(wide * wide, axis=1, keepdims=True)
    inverse = lax.rsqrt(square / depth + 1e-06)
    for n in range(0, depth, width):
        wide = tokens[:, n : n + width].astype(F32)
        normed[:, n : n + width] = (wide * inverse * mg_ref[:, n : n + width]).astype(BF16)

    topk = routes_ref.shape[0]
    table = columns_of([routes_ref[...].astype(F32), rw_ref[...]])
    lane = lax.broadcasted_iota(jnp.int32, (count, 128), 1).astype(F32)
    named = [lane == table[:, k : k + 1] for k in range(topk)]
    member = named[0]
    for k in range(1, topk):
        member = member | named[k]
    earlier = lax.broadcasted_iota(jnp.int32, (count, count), 0) > lax.broadcasted_iota(
        jnp.int32, (count, count), 1
    )
    before = jnp.dot(
        jnp.where(earlier, 1.0, 0.0).astype(BF16),
        jnp.where(member, 1.0, 0.0).astype(BF16),
        preferred_element_type=F32,
    )
    slot_no = lax.broadcasted_iota(jnp.int32, (count, slots), 1).astype(F32)
    place = jnp.zeros((count, slots), F32)
    weight = jnp.zeros((count, slots), F32)
    for k in range(topk):
        ahead = jnp.sum(jnp.where(named[k], before, 0.0), axis=1, keepdims=True)
        hit = slot_no == table[:, k : k + 1] * cap + ahead
        place = jnp.where(hit, 1.0, place)
        weight = jnp.where(hit, table[:, topk + k : topk + k + 1], weight)
    place = place.astype(BF16)
    weight_high, weight_low = split_bf16(weight)

    def stage(side_no):
        for n in range(0, half, width):
            cols = pl.ds(pl.multiple_of(side_no * half + n, width), width)
            moved = lax.dot_general(
                place, normed[:, cols], (((0,), (0,)), ((), ())), preferred_element_type=F32
            ).astype(BF16)
            for x in range(ep_count):
                staged[side_no, x, :, n : n + width] = moved[x * cap : (x + 1) * cap]

    quarter = half // 2
    early = [(0, dy, dx) for dy, dx in around[:1]]
    middle = [(1, dy, dx) for dy, dx in around[:1]]
    late = [(h, dy, dx) for dy, dx in around[1:] for h in range(2)]

    def dx_copy(half_no, peer, origin):
        cols = pl.ds(half_no * quarter, quarter)
        return remote(
            staged.at[core, peer, :, cols],
            arrived.at[core, origin, :, cols],
            dx_s.at[half_no, peer],
            dx_r.at[half_no, origin],
            (peer, t),
        )

    def dp_copy(origin):
        return remote(
            arrived.at[core, origin],
            arrived.at[core, origin],
            dp_s.at[origin],
            dp_r.at[origin],
            (e, 2 * z + 1 - core),
        )

    def dp_other(origin):
        return remote(
            arrived.at[core, origin],
            arrived.at[1 - core, origin],
            dp_s.at[origin],
            dp_r.at[origin],
            (e, 2 * z + 1 - core),
        )

    stage(core)
    for half_no, dy, dx in early:
        dx_copy(half_no, ep_peer(dy, dx), e).start()

    def stacked(ref):
        return jnp.concatenate(
            [ref[h : h + 1, c * CH : (c + 1) * CH] for h in range(heads) for c in range(chunks)],
            axis=0,
        )

    gates = gate_rows(stacked(ig_ref), stacked(fg_ref))
    loads["k"].wait()
    loads["v"].wait()
    summary(heads, chunks, k_ref, v_ref, gates, sums, e)

    def st(peer, origin):
        return remote(
            sums.at[origin], sums.at[origin], st_s.at[peer], st_r.at[origin], (peer, t)
        )

    for dy, dx in around:
        st(ep_peer(dy, dx), e).start()

    stage(1 - core)
    for s in range(2):
        arrived[s, e] = staged[s, e]

    loads["sg"].wait()
    loads["su"].wait()
    gate = jnp.dot(normed[...], sg[...], preferred_element_type=F32)
    up = jnp.dot(normed[...], su[...], preferred_element_type=F32)
    shared_hidden[...] = (gate / (1.0 + jnp.exp(-gate)) * up).astype(BF16)

    for half_no, dy, dx in middle:
        dx_copy(half_no, ep_peer(dy, dx), e).start()

    def line(kind, part, origin, where):
        sems = {"up": (up_s, up_r), "dn": (dn_s, dn_r), "pa": (pa_s, pa_r)}[kind]
        ref = mixed.at[2 * origin + core, pl.ds(part * seg, seg)]
        return remote(
            ref, ref, sems[0].at[part, origin], sems[1].at[part, origin], (e, where)
        )

    def line_other(part, origin):
        ref = mixed.at[2 * origin + 1 - core, pl.ds(part * seg, seg)]
        return remote(
            ref, ref, pa_s.at[part, origin], pa_r.at[part, origin], (e, 2 * z + 1 - core)
        )

    def go_up(part, origin):
        @pl.when(z + 1 < chips)
        def _():
            line("up", part, origin, t + 2).start()

    def go_down(part, origin):
        @pl.when(z > 0)
        def _():
            line("dn", part, origin, t - 2).start()

    def go_across(part, origin):
        line("pa", part, origin, 2 * z + 1 - core).start()

    def after(c):
        if (c + 1) % (chunks // SPLIT) == 0:
            part = (c + 1) // (chunks // SPLIT) - 1
            mixed[t, part * seg : (part + 1) * seg] = own[part * seg : (part + 1) * seg]
            go_up(part, z)
            go_down(part, z)
            go_across(part, z)

    def relay(step, part):
        if step >= chips:
            return

        @pl.when(z >= step)
        def _():
            line("up", part, z - step, t - 2).wait_recv()
            go_up(part, z - step)
            go_across(part, z - step)

        @pl.when(z + step < chips)
        def _():
            line("dn", part, z + step, t + 2).wait_recv()
            go_down(part, z + step)
            go_across(part, z + step)

    for dy, dx in around:
        peer = ep_peer(dy, dx)
        st(peer, peer).wait_recv()
    for half_no, dy, dx in late:
        dx_copy(half_no, ep_peer(dy, dx), e).start()
    loads["q"].wait()
    loads["og"].wait()
    state, stab = entering_state(heads, e, sums)
    cell_blocks(
        heads, chunks, state, stab, gates, q_ref, k_ref, v_ref, og_ref, gain_ref, own, after
    )

    rowwise = [(dy, dx) for dy, dx in around if dy == 0]
    columnwise = [(dy, dx) for dy, dx in around if dx == 0]

    def wx(part, peer, origin):
        ref = wcols.at[pl.ds(part * group, group), origin]
        return remote(ref, ref, wx_s.at[part, peer], wx_r.at[part, origin], (peer, t))

    def wf(part, peer, origin):
        ref = wcols.at[pl.ds(part * group, group), origin]
        return remote(ref, ref, wf_s.at[origin, peer], wx_r.at[part, origin], (peer, t))

    paths = ((rowwise, columnwise), (columnwise, rowwise))

    loads["own"].wait()
    for k in range(1, tp_count):
        wz((t + k) % tp_count, (t + k) % tp_count).wait_recv()
    for part, (near, far) in enumerate(paths):
        for dy, dx in near:
            wx(part, ep_peer(dy, dx), e).start()
    relay(1, 0)
    for dy, dx in around:
        origin = ep_peer(dy, dx)
        for half_no in range(2):
            dx_copy(half_no, origin, origin).wait_recv()
        dp_copy(origin).start()
    for part, (near, far) in enumerate(paths):
        for dy, dx in far:
            wx(part, ep_peer(dy, dx), e).start()
    relay(1, 1)
    for dy, dx in around:
        dp_other(ep_peer(dy, dx)).wait_recv()

    loads["eg"].wait()
    loads["eu"].wait()
    units = eg.shape[1]
    tile = tiles(units, 256)

    def both(weights, n):
        return sum(
            jnp.dot(
                arrived[s].reshape(slots, half),
                weights[s * half : (s + 1) * half, n : n + tile],
                preferred_element_type=F32,
            )
            for s in range(2)
        )

    for n in range(0, units, tile):
        gate = both(eg, n)
        up = both(eu, n)
        hidden[:, n : n + tile] = (gate / (1.0 + jnp.exp(-gate)) * up).astype(BF16)

    loads["ed"].wait()
    loads["sd"].wait()

    def pp(block):
        return remote(
            give.at[block], take.at[block], pp_s.at[block], pp_r.at[block],
            (e, 2 * z + 1 - core),
        )

    def products(place_no, owner):
        cols = pl.ds(pl.multiple_of((2 * order[place_no] + owner) * feat, feat), feat)
        return (
            jnp.dot(hidden[...], ed[:, cols], preferred_element_type=F32),
            jnp.dot(shared_hidden[...], sd[:, cols], preferred_element_type=F32),
        )

    for block in range(chips):
        routed, common = products(block, 1 - core)
        give[block, 0:slots] = routed.astype(BF16)
        give[block, slots:] = common.astype(BF16)
        pp(block).start()
    relay(2, 0)

    def rt(part, peer, origin):
        blocks = pl.ds(part * batch, batch)
        return remote(
            reduced.at[blocks, peer],
            returned.at[blocks, origin],
            rt_s.at[part, peer],
            rt_r.at[part, origin],
            (peer, t),
        )

    for block in range(chips):
        routed, common = products(block, core)
        pp(block).wait_recv()
        total = (routed + take[block, 0:slots].astype(F32)).astype(BF16)
        for x in range(ep_count):
            reduced[block, x] = total[x * cap : (x + 1) * cap]
        shared_own[block] = common + take[block, slots:].astype(F32)
        if (block + 1) % batch == 0:
            for dy, dx in around:
                rt(block // batch, ep_peer(dy, dx), e).start()
    for block in range(chips):
        returned[block, e] = reduced[block, e]
    relay(2, 1)
    for part, (near, far) in enumerate(paths):
        for dy, dx in near:
            origin = ep_peer(dy, dx)
            wx(part, origin, origin).wait_recv()
            for fy, fx in far:
                wf(part, ep_peer(fy, fx), origin).start()

    def zs(to, origin):
        return remote(
            part_out.at[to], part_in.at[origin], zs_s.at[to], zs_r.at[origin], (e, 2 * to + core)
        )

    for part in range(SPLIT):
        for dy, dx in around:
            origin = ep_peer(dy, dx)
            rt(part, origin, origin).wait_recv()
        for place_no in range(part * batch, (part + 1) * batch):
            block = order[place_no]
            results = returned[place_no].reshape(slots, feat)
            total = (
                jnp.dot(weight_high, results, preferred_element_type=F32)
                + jnp.dot(weight_low, results, preferred_element_type=F32)
                + shared_own[place_no]
            )
            part_out[block] = total.astype(BF16)

            @pl.when(z == block)
            def _():
                final[...] = total

            @pl.when(z != block)
            def _():
                zs(block, z).start()

        for step in range(3, chips):
            relay(step, part)

    for k in range(1, tp_count):
        wz((t + k) % tp_count, t).wait_send()
    for dy, dx in rowwise + columnwise:
        for part in range(SPLIT):
            wx(part, ep_peer(dy, dx), e).wait_send()
    for dy, dx in around:
        peer = ep_peer(dy, dx)
        st(peer, e).wait_send()
        for half_no in range(2):
            dx_copy(half_no, peer, e).wait_send()
        dp_copy(peer).wait_send()
        for part in range(SPLIT):
            rt(part, peer, e).wait_send()
    for block in range(chips):
        pp(block).wait_send()
    for part in range(SPLIT):
        for origin in range(chips):
            line("pa", part, origin, 2 * z + 1 - core).wait_send()

            @pl.when((origin <= z) & (z + 1 < chips))
            def _():
                line("up", part, origin, t + 2).wait_send()

            @pl.when((origin >= z) & (z > 0))
            def _():
                line("dn", part, origin, t - 2).wait_send()

    for dy, dx in around:
        origin = ep_peer(dy, dx)
        if dy == 0:
            wx(1, origin, origin).wait_recv()
        elif dx == 0:
            wx(0, origin, origin).wait_recv()
        else:
            for part in range(SPLIT):
                wx(part, origin, origin).wait_recv()
    for part in range(SPLIT):
        for origin in range(chips):
            line_other(part, origin).wait_recv()
    step_rows = tiles(tok, 256)

    @pl.loop(0, tok // step_rows)
    def _(i):
        rows = pl.ds(pl.multiple_of(i * step_rows, step_rows), step_rows)
        total = 0.0
        for b in range(tp_count):
            total = total + jnp.dot(
                mixed[b, rows],
                wcols[b].reshape(ep_count * share, feat),
                preferred_element_type=F32,
            )
        out_rows[rows] = total
        pltpu.make_async_copy(out_rows.at[rows], mixer_out.at[rows], out_sem.at[i]).start()

    total = final[...]
    for k in range(1, chips):
        origin = (z + k) % chips
        zs(origin, origin).wait_recv()
        total = total + part_in[origin].astype(F32)
    own_rows[...] = total
    own_copy = pltpu.make_async_copy(own_rows, moe_out, load_sem.at[len(loads)])
    own_copy.start()

    for part, (near, far) in enumerate(paths):
        for dy, dx in near:
            for fy, fx in far:
                wf(part, ep_peer(fy, fx), ep_peer(dy, dx)).wait_send()
    for block in range(chips):

        @pl.when(z != block)
        def _():
            zs(block, z).wait_send()

    @pl.loop(0, tok // step_rows)
    def _(i):
        rows = pl.ds(pl.multiple_of(i * step_rows, step_rows), step_rows)
        pltpu.make_async_copy(out_rows.at[rows], mixer_out.at[rows], out_sem.at[i]).wait()

    own_copy.wait()


def local(
    queries,
    keys,
    values,
    out_gate,
    in_gate,
    forget_gate,
    out_gain,
    out_weight,
    moe_rows,
    moe_gain,
    routes,
    route_weight,
    expert_gate,
    expert_up,
    expert_down,
    shared_gate,
    shared_up,
    shared_down,
):
    tp_count = lax.axis_size("tp")
    ep_count = lax.axis_size("ep")
    count, depth = moe_rows.shape
    assert expert_gate.shape[0] == 1
    cap = 3 * count * routes.shape[1] // (2 * ep_count)
    slots = ep_count * cap
    heads = in_gate.shape[0]
    tok = queries.shape[0]
    held = heads * DK
    extra = -(-(1 + 2 * heads) // 8) * 8
    chips = tp_count // 2
    units, common = expert_gate.shape[2], shared_gate.shape[1]
    wide, features = out_weight.shape
    feat = features // tp_count
    share = wide // ep_count
    half = depth // 2
    side = 1
    while side * side < ep_count:
        side *= 2
    dma = pltpu.SemaphoreType.DMA

    def vm(*shape, dtype=BF16):
        return pltpu.VMEM(shape, dtype)

    scratch = [
        vm(ep_count, held + extra, 128, dtype=F32),
        vm(tok, heads * DV),
        vm(tp_count, tok, heads * DV),
        vm(tp_count, ep_count, share, feat),
        vm(tok, feat, dtype=F32),
        vm(count, depth),
        vm(tok, held),
        vm(tok, held),
        vm(tok, heads * DV),
        vm(tok, heads * DV),
        vm(count, depth),
        vm(2, ep_count, cap, half),
        vm(2, ep_count, cap, half),
        vm(depth, units),
        vm(depth, units),
        vm(units, depth),
        vm(depth, common),
        vm(depth, common),
        vm(common, depth),
        vm(slots, units),
        vm(count, common),
        vm(chips, slots + count, feat),
        vm(chips, slots + count, feat),
        vm(chips, ep_count, cap, feat),
        vm(chips, ep_count, cap, feat),
        vm(chips, count, feat, dtype=F32),
        vm(chips, count, feat),
        vm(chips, count, feat),
        vm(count, feat, dtype=F32),
        vm(count, feat, dtype=F32),
        dma((13,)),
        dma((-(-tok // 256),)),
    ]
    scratch += [dma((tp_count,))] * 2
    scratch += [dma((SPLIT, ep_count))] * 2
    scratch += [dma((ep_count, ep_count))]
    scratch += [dma((ep_count,))] * 2
    scratch += [dma((2, ep_count))] * 2
    scratch += [dma((ep_count,))] * 2
    scratch += [dma((SPLIT, chips))] * 6
    scratch += [dma((chips,))] * 2
    scratch += [dma((SPLIT, ep_count))] * 2
    scratch += [dma((chips,))] * 2
    mixer_sum, moe_sum = pl.pallas_call(
        functools.partial(step_kernel, ep_count, tp_count, side, cap),
        out_shape=(
            jax.ShapeDtypeStruct((tok, feat), F32),
            jax.ShapeDtypeStruct((count, feat), F32),
        ),
        in_specs=[VM] * 6 + [ANY] * 12,
        out_specs=(ANY, ANY),
        scratch_shapes=scratch,
        compiler_params=pltpu.CompilerParams(
            collective_id=0, has_side_effects=True, vmem_limit_bytes=60 * 1024 * 1024
        ),
        cost_estimate=pl.CostEstimate(
            flops=9_000_000_000, bytes_accessed=30_000_000, transcendentals=0
        ),
    )(
        in_gate,
        forget_gate,
        out_gain.reshape(1, -1),
        moe_gain.reshape(1, -1),
        routes.T,
        route_weight.T,
        queries,
        keys,
        values,
        out_gate,
        moe_rows,
        out_weight,
        expert_gate,
        expert_up,
        expert_down,
        shared_gate,
        shared_up,
        shared_down,
    )
    return mixer_sum.astype(BF16), moe_sum.astype(BF16)


def solution(mesh):
    return jax.shard_map(
        local,
        mesh=mesh,
        in_specs=(
            P("ep", "tp"),
            P("ep", "tp"),
            P("ep", "tp"),
            P("ep", "tp"),
            P("tp", "ep"),
            P("tp", "ep"),
            P("tp"),
            P("tp", None),
            P("ep", None),
            P(),
            P("ep", None),
            P("ep", None),
            P("ep", None, "tp"),
            P("ep", None, "tp"),
            P("ep", "tp", None),
            P(None, "tp"),
            P(None, "tp"),
            P("tp", None),
        ),
        out_specs=(P("ep", "tp"), P("ep", "tp")),
        check_vma=False,
    )
```

```python
import functools

import jax
import jax.numpy as jnp
from jax import lax
from jax.experimental import pallas as pl
from jax.experimental.pallas import tpu as pltpu
from jax.sharding import PartitionSpec as P

DK = 64
DV = 128
CH = 128
F32 = jnp.float32
BF16 = jnp.bfloat16
VM = pl.BlockSpec(memory_space=pltpu.VMEM)
ANY = pl.BlockSpec(memory_space=pl.ANY)
MESH = pl.DeviceIdType.MESH
SPLIT = 2


def gate_rows(ig, fg):
    lane = lax.broadcasted_iota(jnp.int32, ig.shape, 1)
    total = jnp.minimum(fg, 0.0) - jnp.log1p(jnp.exp(-jnp.abs(fg)))
    step = 1
    while step < CH:
        total = total + jnp.where(lane >= step, pltpu.roll(total, step, 1), 0.0)
        step *= 2
    level = ig - total
    top = level
    step = 1
    while step < CH:
        top = jnp.maximum(top, jnp.where(lane >= step, pltpu.roll(top, step, 1), -1e30))
        step *= 2
    return total, level, top


def columns_of(parts):
    rows = sum(part.shape[0] for part in parts)
    padded = -(-rows // 128) * 128
    if padded > rows:
        parts = list(parts) + [jnp.zeros((padded - rows, CH), F32)]
    return jnp.concatenate(parts, axis=0).T


def split_bf16(x):
    high = x.astype(BF16)
    return high, (x - high.astype(F32)).astype(BF16)


def weighted_keys(keys, cols, first, heads, chunks):
    lane_head = lax.broadcasted_iota(jnp.int32, keys.shape, 1) // DK
    weight = jnp.broadcast_to(cols[:, first : first + 1], keys.shape)
    for h in range(1, heads):
        at = first + h * chunks
        weight = jnp.where(lane_head == h, jnp.broadcast_to(cols[:, at : at + 1], keys.shape), weight)
    return split_bf16(keys.astype(F32) * weight)


def add_outer(kw, values):
    dims = (((0,), (0,)), ((), ()))
    return lax.dot_general(kw[0], values, dims, preferred_element_type=F32) + lax.dot_general(
        kw[1], values, dims, preferred_element_type=F32
    )


def pick_head(parts, shape, axis):
    head = lax.broadcasted_iota(jnp.int32, shape, axis) // DK
    out = jnp.broadcast_to(parts[0], shape)
    for h in range(1, len(parts)):
        out = jnp.where(head == h, jnp.broadcast_to(parts[h], shape), out)
    return out


def summary(heads, chunks, k_ref, v_ref, gates, out_ref, slot):
    width = heads * DK
    total, level, top = gates
    shape = total.shape
    chunk = lax.broadcasted_iota(jnp.int32, shape, 0) % chunks
    last = jnp.broadcast_to(total[:, CH - 1 : CH], shape)
    suffix = last
    step = 1
    while step < chunks:
        moved = pltpu.roll(suffix, shape[0] - step, 0)
        suffix = suffix + jnp.where(chunk + step < chunks, moved, 0.0)
        step *= 2
    reach = suffix + jnp.broadcast_to(top[:, CH - 1 : CH], shape)
    tops = [
        jnp.max(reach[h * chunks : (h + 1) * chunks], axis=0, keepdims=True) for h in range(heads)
    ]
    weight = [
        jnp.exp(
            level[h * chunks : (h + 1) * chunks] + suffix[h * chunks : (h + 1) * chunks] - tops[h]
        )
        for h in range(heads)
    ]
    cols = columns_of(weight)
    state = jnp.zeros((width, heads * DV + 128), F32)
    for c in range(chunks):
        rows = pl.ds(c * CH, CH)
        kw = weighted_keys(k_ref[rows, :], cols, c, heads, chunks)
        values = jnp.concatenate([v_ref[rows, :], jnp.ones((CH, 128), BF16)], axis=1)
        state = state + add_outer(kw, values)
    out_ref[slot] = jnp.zeros(out_ref.shape[1:], F32)
    out_ref[slot, 0:width, :] = pick_head(
        [state[:, h * DV : (h + 1) * DV] for h in range(heads)], (width, DV), 0
    )
    normal = state[:, heads * DV :].T
    out_ref[slot, width : width + 1, 0:width] = normal[0:1, :]
    for h in range(heads):
        out_ref[slot, width + 1 + h : width + 2 + h, :] = tops[h]
        at = width + 1 + heads + h
        out_ref[slot, at : at + 1, :] = suffix[h * chunks : h * chunks + 1]


def entering_state(heads, pos, sum_ref):
    width = heads * DK
    matrix = jnp.zeros((width, DV), F32)
    normal = jnp.zeros((1, width), F32)
    stab = [jnp.zeros((1, 128), F32) for _ in range(heads)]
    for e in range(sum_ref.shape[0]):
        reached = e < pos
        part = sum_ref.at[e]
        old_w, new_w, new_stab = [], [], []
        for h in range(heads):
            at = width + 1 + h
            carried = part[at + heads : at + heads + 1, :] + stab[h]
            there = part[at : at + 1, :]
            joined = jnp.maximum(carried, there)
            old_w.append(jnp.where(reached, jnp.exp(carried - joined), 1.0))
            new_w.append(jnp.where(reached, jnp.exp(there - joined), 0.0))
            new_stab.append(jnp.where(reached, joined, stab[h]))
        matrix = (
            pick_head(old_w, (width, DV), 0) * matrix
            + pick_head(new_w, (width, DV), 0) * part[0:width, :]
        )
        normal = (
            pick_head([w[:, 0:width] for w in old_w], (1, width), 1) * normal
            + pick_head([w[:, 0:width] for w in new_w], (1, width), 1)
            * part[width : width + 1, 0:width]
        )
        stab = new_stab
    normal_cols = jnp.broadcast_to(normal, (128, width)).T
    return jnp.concatenate([matrix] * heads + [normal_cols], axis=1), stab


def cell_blocks(
    heads, chunks, state, stab, gates, q_ref, k_ref, v_ref, og_ref, gain_ref, out_ref, after
):
    width = heads * DK
    total, level, top = gates
    shape = total.shape
    last = jnp.broadcast_to(total[:, CH - 1 : CH], shape)
    last_top = jnp.broadcast_to(top[:, CH - 1 : CH], shape)
    entering, leaving = [], []
    for h in range(heads):
        now = stab[h]
        for c in range(chunks):
            r = h * chunks + c
            entering.append(now)
            now = last[r : r + 1] + jnp.maximum(now, last_top[r : r + 1])
            leaving.append(now)
    entering = jnp.concatenate(entering, axis=0)
    leaving = jnp.concatenate(leaving, axis=0)
    peak = jnp.maximum(top, entering)
    decay = jnp.exp(last + entering - leaving)
    count = heads * chunks
    cols = columns_of(
        [
            peak,
            jnp.exp(entering - peak),
            jnp.exp(-(total + peak)),
            jnp.exp(last + level - leaving),
        ]
    )
    causal = lax.broadcasted_iota(jnp.int32, (CH, CH), 0) >= lax.broadcasted_iota(
        jnp.int32, (CH, CH), 1
    )
    lane_head = lax.broadcasted_iota(jnp.int32, (CH, width), 1) // DK
    for c in range(chunks):
        rows = pl.ds(c * CH, CH)
        keys = k_ref[rows, :]
        values = v_ref[rows, :]
        queries = q_ref[rows, :] * jnp.asarray(DK**-0.5, BF16)
        high, low = split_bf16(state)
        for h in range(heads):
            r = h * chunks + c
            mine = jnp.where(lane_head == h, queries, jnp.zeros_like(queries))
            raw = lax.dot_general(
                mine, keys, (((1,), (1,)), ((), ())), preferred_element_type=F32
            )
            logs = level[r : r + 1, :] - cols[:, r : r + 1]
            scores = raw * jnp.exp(jnp.where(causal, logs, -jnp.inf))
            inner = jnp.dot(
                scores.astype(BF16), values[:, h * DV : (h + 1) * DV], preferred_element_type=F32
            )
            across = 0.0
            for piece in (high, low):
                rhs = jnp.concatenate(
                    [piece[:, h * DV : (h + 1) * DV], piece[:, heads * DV :]], axis=1
                )
                across = across + jnp.dot(mine, rhs, preferred_element_type=F32)
            inter = cols[:, count + r : count + r + 1]
            signed = jnp.sum(scores, axis=1, keepdims=True) + inter * across[:, DV : DV + 1]
            divisor = jnp.maximum(jnp.abs(signed), cols[:, 2 * count + r : 2 * count + r + 1])
            cells = (inner + inter * across[:, :DV]) * (1.0 / divisor)
            at = slice(h * DV, (h + 1) * DV)
            gate = og_ref[rows, at].astype(F32)
            out_ref[rows, at] = (cells / (1.0 + jnp.exp(-gate)) * gain_ref[:, at]).astype(BF16)
        if c + 1 < chunks:
            kw = weighted_keys(keys, cols, 3 * count + c, heads, chunks)
            scale = pick_head(
                [decay[h * chunks + c : h * chunks + c + 1] for h in range(heads)], (width, 128), 0
            )
            rhs = jnp.concatenate([values, jnp.ones((CH, 128), BF16)], axis=1)
            state = state * jnp.concatenate([scale] * (heads + 1), axis=1) + add_outer(kw, rhs)
        after(c)


def tiles(width, most):
    return min(width, most)


def step_kernel(
    ep_count,
    tp_count,
    side,
    cap,
    ig_ref,
    fg_ref,
    gain_ref,
    mg_ref,
    routes_ref,
    rw_ref,
    q_hbm,
    k_hbm,
    v_hbm,
    og_hbm,
    rows_hbm,
    ow_hbm,
    eg_hbm,
    eu_hbm,
    ed_hbm,
    sg_hbm,
    su_hbm,
    sd_hbm,
    mixer_out,
    moe_out,
    sums,
    own,
    mixed,
    wcols,
    out_rows,
    tokens,
    q_ref,
    k_ref,
    v_ref,
    og_ref,
    normed,
    staged,
    arrived,
    eg,
    eu,
    ed,
    sg,
    su,
    sd,
    hidden,
    shared_hidden,
    give,
    take,
    reduced,
    returned,
    shared_own,
    part_out,
    part_in,
    final,
    own_rows,
    load_sem,
    out_sem,
    wz_s,
    wz_r,
    wx_s,
    wx_r,
    wf_s,
    wf_r,
    st_s,
    st_r,
    dx_s,
    dx_r,
    dp_s,
    dp_r,
    up_s,
    up_r,
    dn_s,
    dn_r,
    pa_s,
    pa_r,
    pp_s,
    pp_r,
    rt_s,
    rt_r,
    zs_s,
    zs_r,
):
    e, t = lax.axis_index("ep"), lax.axis_index("tp")
    z, core = t // 2, t % 2
    chips = tp_count // 2
    heads = ig_ref.shape[0]
    tok = q_ref.shape[0]
    chunks = tok // CH
    count, depth = tokens.shape
    half = depth // 2
    feat = mixer_out.shape[1]
    share = wcols.shape[2]
    slots = ep_count * cap
    group = tp_count // SPLIT
    batch = chips // SPLIT
    order = [b for i in range(chips // 2) for b in (i, chips - 1 - i)]
    seg = tok // SPLIT

    def ep_peer(dy, dx):
        deep = ep_count // side
        return ((e // side + dy) % deep) * side + (e % side + dx) % side

    around = [(dy, dx) for dy in range(ep_count // side) for dx in range(side)][1:]
    around = around[::-1]

    def remote(src, dst, send, recv, where):
        return pltpu.make_async_remote_copy(
            src_ref=src, dst_ref=dst, send_sem=send, recv_sem=recv, device_id=where,
            device_id_type=MESH,
        )

    barrier = pltpu.get_barrier_semaphore()
    for dy, dx in around:
        pl.semaphore_signal(barrier, inc=1, device_id=(ep_peer(dy, dx), t), device_id_type=MESH)
    for k in range(1, tp_count):
        pl.semaphore_signal(
            barrier, inc=1, device_id=(e, (t + k) % tp_count), device_id_type=MESH
        )
    loads = {}
    for name, src, dst in (
        ("tokens", rows_hbm, tokens),
        ("k", k_hbm, k_ref),
        ("v", v_hbm, v_ref),
        ("sg", sg_hbm, sg),
        ("su", su_hbm, su),
        ("q", q_hbm, q_ref),
        ("og", og_hbm, og_ref),
        (
            "own",
            ow_hbm.at[
                pl.ds(pl.multiple_of(e * share, share), share),
                pl.ds(pl.multiple_of(t * feat, feat), feat),
            ],
            wcols.at[t, e],
        ),
        ("eg", eg_hbm.at[0], eg),
        ("eu", eu_hbm.at[0], eu),
        ("ed", ed_hbm.at[0], ed),
        ("sd", sd_hbm, sd),
    ):
        loads[name] = pltpu.make_async_copy(src, dst, load_sem.at[len(loads)])
        loads[name].start()
    pl.semaphore_wait(barrier, ep_count - 1 + tp_count - 1)

    def wz(to, origin):
        return remote(
            ow_hbm.at[
                pl.ds(pl.multiple_of(e * share, share), share),
                pl.ds(pl.multiple_of(to * feat, feat), feat),
            ],
            wcols.at[origin, e],
            wz_s.at[to],
            wz_r.at[origin],
            (e, to),
        )

    for k in range(1, tp_count):
        wz((t + k) % tp_count, t).start()

    loads["tokens"].wait()
    width = tiles(half, 512)
    square = jnp.zeros((count, 1), F32)
    for n in range(0, depth, width):
        wide = tokens[:, n : n + width].astype(F32)
        square = square + jnp.sum(wide * wide, axis=1, keepdims=True)
    inverse = lax.rsqrt(square / depth + 1e-06)
    for n in range(0, depth, width):
        wide = tokens[:, n : n + width].astype(F32)
        normed[:, n : n + width] = (wide * inverse * mg_ref[:, n : n + width]).astype(BF16)

    topk = routes_ref.shape[0]
    table = columns_of([routes_ref[...].astype(F32), rw_ref[...]])
    lane = lax.broadcasted_iota(jnp.int32, (count, 128), 1).astype(F32)
    named = [lane == table[:, k : k + 1] for k in range(topk)]
    member = named[0]
    for k in range(1, topk):
        member = member | named[k]
    earlier = lax.broadcasted_iota(jnp.int32, (count, count), 0) > lax.broadcasted_iota(
        jnp.int32, (count, count), 1
    )
    before = jnp.dot(
        jnp.where(earlier, 1.0, 0.0).astype(BF16),
        jnp.where(member, 1.0, 0.0).astype(BF16),
        preferred_element_type=F32,
    )
    slot_no = lax.broadcasted_iota(jnp.int32, (count, slots), 1).astype(F32)
    place = jnp.zeros((count, slots), F32)
    weight = jnp.zeros((count, slots), F32)
    for k in range(topk):
        ahead = jnp.sum(jnp.where(named[k], before, 0.0), axis=1, keepdims=True)
        hit = slot_no == table[:, k : k + 1] * cap + ahead
        place = jnp.where(hit, 1.0, place)
        weight = jnp.where(hit, table[:, topk + k : topk + k + 1], weight)
    place = place.astype(BF16)
    weight_high, weight_low = split_bf16(weight)

    def stage(side_no):
        for n in range(0, half, width):
            cols = pl.ds(pl.multiple_of(side_no * half + n, width), width)
            moved = lax.dot_general(
                place, normed[:, cols], (((0,), (0,)), ((), ())), preferred_element_type=F32
            ).astype(BF16)
            for x in range(ep_count):
                staged[side_no, x, :, n : n + width] = moved[x * cap : (x + 1) * cap]

    quarter = half // 2
    early = [(0, dy, dx) for dy, dx in around[:1]]
    middle = [(1, dy, dx) for dy, dx in around[:1]]
    late = [(h, dy, dx) for dy, dx in around[1:] for h in range(2)]

    def dx_copy(half_no, peer, origin):
        cols = pl.ds(half_no * quarter, quarter)
        return remote(
            staged.at[core, peer, :, cols],
            arrived.at[core, origin, :, cols],
            dx_s.at[half_no, peer],
            dx_r.at[half_no, origin],
            (peer, t),
        )

    def dp_copy(origin):
        return remote(
            arrived.at[core, origin],
            arrived.at[core, origin],
            dp_s.at[origin],
            dp_r.at[origin],
            (e, 2 * z + 1 - core),
        )

    def dp_other(origin):
        return remote(
            arrived.at[core, origin],
            arrived.at[1 - core, origin],
            dp_s.at[origin],
            dp_r.at[origin],
            (e, 2 * z + 1 - core),
        )

    stage(core)
    for half_no, dy, dx in early:
        dx_copy(half_no, ep_peer(dy, dx), e).start()

    def stacked(ref):
        return jnp.concatenate(
            [ref[h : h + 1, c * CH : (c + 1) * CH] for h in range(heads) for c in range(chunks)],
            axis=0,
        )

    gates = gate_rows(stacked(ig_ref), stacked(fg_ref))
    loads["k"].wait()
    loads["v"].wait()
    summary(heads, chunks, k_ref, v_ref, gates, sums, e)

    def st(peer, origin):
        return remote(
            sums.at[origin], sums.at[origin], st_s.at[peer], st_r.at[origin], (peer, t)
        )

    for dy, dx in around:
        st(ep_peer(dy, dx), e).start()

    stage(1 - core)
    for s in range(2):
        arrived[s, e] = staged[s, e]

    loads["sg"].wait()
    loads["su"].wait()
    gate = jnp.dot(normed[...], sg[...], preferred_element_type=F32)
    up = jnp.dot(normed[...], su[...], preferred_element_type=F32)
    shared_hidden[...] = (gate / (1.0 + jnp.exp(-gate)) * up).astype(BF16)

    for half_no, dy, dx in middle:
        dx_copy(half_no, ep_peer(dy, dx), e).start()

    def line(kind, part, origin, where):
        sems = {"up": (up_s, up_r), "dn": (dn_s, dn_r), "pa": (pa_s, pa_r)}[kind]
        ref = mixed.at[2 * origin + core, pl.ds(part * seg, seg)]
        return remote(
            ref, ref, sems[0].at[part, origin], sems[1].at[part, origin], (e, where)
        )

    def line_other(part, origin):
        ref = mixed.at[2 * origin + 1 - core, pl.ds(part * seg, seg)]
        return remote(
            ref, ref, pa_s.at[part, origin], pa_r.at[part, origin], (e, 2 * z + 1 - core)
        )

    def go_up(part, origin):
        @pl.when(z + 1 < chips)
        def _():
            line("up", part, origin, t + 2).start()

    def go_down(part, origin):
        @pl.when(z > 0)
        def _():
            line("dn", part, origin, t - 2).start()

    def go_across(part, origin):
        line("pa", part, origin, 2 * z + 1 - core).start()

    def after(c):
        if (c + 1) % (chunks // SPLIT) == 0:
            part = (c + 1) // (chunks // SPLIT) - 1
            mixed[t, part * seg : (part + 1) * seg] = own[part * seg : (part + 1) * seg]
            go_up(part, z)
            go_down(part, z)
            go_across(part, z)

    def relay(step, part):
        if step >= chips:
            return

        @pl.when(z >= step)
        def _():
            line("up", part, z - step, t - 2).wait_recv()
            go_up(part, z - step)
            go_across(part, z - step)

        @pl.when(z + step < chips)
        def _():
            line("dn", part, z + step, t + 2).wait_recv()
            go_down(part, z + step)
            go_across(part, z + step)

    for dy, dx in around:
        peer = ep_peer(dy, dx)
        st(peer, peer).wait_recv()
    for half_no, dy, dx in late:
        dx_copy(half_no, ep_peer(dy, dx), e).start()
    loads["q"].wait()
    loads["og"].wait()
    state, stab = entering_state(heads, e, sums)
    cell_blocks(
        heads, chunks, state, stab, gates, q_ref, k_ref, v_ref, og_ref, gain_ref, own, after
    )

    rowwise = [(dy, dx) for dy, dx in around if dy == 0]
    columnwise = [(dy, dx) for dy, dx in around if dx == 0]

    def wx(part, peer, origin):
        ref = wcols.at[pl.ds(part * group, group), origin]
        return remote(ref, ref, wx_s.at[part, peer], wx_r.at[part, origin], (peer, t))

    columns = feat // 2

    def wf(part, cut, peer, origin):
        ref = wcols.at[pl.ds(part * group, group), origin, :, pl.ds(cut * columns, columns)]
        return remote(
            ref, ref, wf_s.at[cut, origin, peer], wf_r.at[cut, part, origin], (peer, t)
        )

    paths = ((rowwise, columnwise), (columnwise, rowwise))

    loads["own"].wait()
    for k in range(1, tp_count):
        wz((t + k) % tp_count, (t + k) % tp_count).wait_recv()
    for part, (near, far) in enumerate(paths):
        for dy, dx in near:
            wx(part, ep_peer(dy, dx), e).start()
    relay(1, 0)
    for dy, dx in around:
        origin = ep_peer(dy, dx)
        for half_no in range(2):
            dx_copy(half_no, origin, origin).wait_recv()
        dp_copy(origin).start()
    for part, (near, far) in enumerate(paths):
        for dy, dx in far:
            wx(part, ep_peer(dy, dx), e).start()
    relay(1, 1)
    for dy, dx in around:
        dp_other(ep_peer(dy, dx)).wait_recv()

    loads["eg"].wait()
    loads["eu"].wait()
    units = eg.shape[1]
    tile = tiles(units, 256)

    def both(weights, n):
        return sum(
            jnp.dot(
                arrived[s].reshape(slots, half),
                weights[s * half : (s + 1) * half, n : n + tile],
                preferred_element_type=F32,
            )
            for s in range(2)
        )

    for n in range(0, units, tile):
        gate = both(eg, n)
        up = both(eu, n)
        hidden[:, n : n + tile] = (gate / (1.0 + jnp.exp(-gate)) * up).astype(BF16)

    loads["ed"].wait()
    loads["sd"].wait()

    def pp(block):
        return remote(
            give.at[block], take.at[block], pp_s.at[block], pp_r.at[block],
            (e, 2 * z + 1 - core),
        )

    def products(place_no, owner):
        cols = pl.ds(pl.multiple_of((2 * order[place_no] + owner) * feat, feat), feat)
        return (
            jnp.dot(hidden[...], ed[:, cols], preferred_element_type=F32),
            jnp.dot(shared_hidden[...], sd[:, cols], preferred_element_type=F32),
        )

    for block in range(chips):
        routed, common = products(block, 1 - core)
        give[block, 0:slots] = routed.astype(BF16)
        give[block, slots:] = common.astype(BF16)
        pp(block).start()
    relay(2, 0)

    def rt(part, peer, origin):
        blocks = pl.ds(part * batch, batch)
        return remote(
            reduced.at[blocks, peer],
            returned.at[blocks, origin],
            rt_s.at[part, peer],
            rt_r.at[part, origin],
            (peer, t),
        )

    for block in range(chips):
        routed, common = products(block, core)
        pp(block).wait_recv()
        total = (routed + take[block, 0:slots].astype(F32)).astype(BF16)
        for x in range(ep_count):
            reduced[block, x] = total[x * cap : (x + 1) * cap]
        shared_own[block] = common + take[block, slots:].astype(F32)
        if (block + 1) % batch == 0:
            for dy, dx in around:
                rt(block // batch, ep_peer(dy, dx), e).start()
    for block in range(chips):
        returned[block, e] = reduced[block, e]
    relay(2, 1)
    for cut in range(2):
        for part, (near, far) in enumerate(paths):
            for dy, dx in near:
                origin = ep_peer(dy, dx)
                if cut == 0:
                    wx(part, origin, origin).wait_recv()
                for fy, fx in far:
                    wf(part, cut, ep_peer(fy, fx), origin).start()

    def zs(to, origin):
        return remote(
            part_out.at[to], part_in.at[origin], zs_s.at[to], zs_r.at[origin], (e, 2 * to + core)
        )

    for part in range(SPLIT):
        for dy, dx in around:
            origin = ep_peer(dy, dx)
            rt(part, origin, origin).wait_recv()
        for place_no in range(part * batch, (part + 1) * batch):
            block = order[place_no]
            results = returned[place_no].reshape(slots, feat)
            total = (
                jnp.dot(weight_high, results, preferred_element_type=F32)
                + jnp.dot(weight_low, results, preferred_element_type=F32)
                + shared_own[place_no]
            )
            part_out[block] = total.astype(BF16)

            @pl.when(z == block)
            def _():
                final[...] = total

            @pl.when(z != block)
            def _():
                zs(block, z).start()

        for step in range(3, chips):
            relay(step, part)

    for k in range(1, tp_count):
        wz((t + k) % tp_count, t).wait_send()
    for dy, dx in rowwise + columnwise:
        for part in range(SPLIT):
            wx(part, ep_peer(dy, dx), e).wait_send()
    for dy, dx in around:
        peer = ep_peer(dy, dx)
        st(peer, e).wait_send()
        for half_no in range(2):
            dx_copy(half_no, peer, e).wait_send()
        dp_copy(peer).wait_send()
        for part in range(SPLIT):
            rt(part, peer, e).wait_send()
    for block in range(chips):
        pp(block).wait_send()
    for part in range(SPLIT):
        for origin in range(chips):
            line("pa", part, origin, 2 * z + 1 - core).wait_send()

            @pl.when((origin <= z) & (z + 1 < chips))
            def _():
                line("up", part, origin, t + 2).wait_send()

            @pl.when((origin >= z) & (z > 0))
            def _():
                line("dn", part, origin, t - 2).wait_send()

    for dy, dx in around:
        origin = ep_peer(dy, dx)
        if dy == 0:
            wx(1, origin, origin).wait_recv()
        elif dx == 0:
            wx(0, origin, origin).wait_recv()
    for part in range(SPLIT):
        for origin in range(chips):
            line_other(part, origin).wait_recv()
    step_rows = tiles(tok, 256)

    for cut in range(2):
        for dy, dx in around:
            if dy and dx:
                for part in range(SPLIT):
                    origin = ep_peer(dy, dx)
                    wf(part, cut, origin, origin).wait_recv()
        cols = pl.ds(cut * columns, columns)

        @pl.loop(0, tok // step_rows)
        def _(i):
            rows = pl.ds(pl.multiple_of(i * step_rows, step_rows), step_rows)
            total = 0.0
            for b in range(tp_count):
                total = total + jnp.dot(
                    mixed[b, rows],
                    wcols[b, :, :, cut * columns : (cut + 1) * columns].reshape(
                        ep_count * share, columns
                    ),
                    preferred_element_type=F32,
                )
            out_rows[rows, cols] = total.astype(BF16)
            pltpu.make_async_copy(
                out_rows.at[rows, cols], mixer_out.at[rows, cols], out_sem.at[cut, i]
            ).start()

    total = final[...]
    for k in range(1, chips):
        origin = (z + k) % chips
        zs(origin, origin).wait_recv()
        total = total + part_in[origin].astype(F32)
    own_rows[...] = total.astype(BF16)
    own_copy = pltpu.make_async_copy(own_rows, moe_out, load_sem.at[len(loads)])
    own_copy.start()

    for part, (near, far) in enumerate(paths):
        for dy, dx in near:
            for fy, fx in far:
                for cut in range(2):
                    wf(part, cut, ep_peer(fy, fx), ep_peer(dy, dx)).wait_send()
    for block in range(chips):

        @pl.when(z != block)
        def _():
            zs(block, z).wait_send()

    for cut in range(2):
        cols = pl.ds(cut * columns, columns)

        @pl.loop(0, tok // step_rows)
        def _(i):
            rows = pl.ds(pl.multiple_of(i * step_rows, step_rows), step_rows)
            pltpu.make_async_copy(
                out_rows.at[rows, cols], mixer_out.at[rows, cols], out_sem.at[cut, i]
            ).wait()

    own_copy.wait()


def hand_over(pieces, a_ref, b_ref, a_out, b_out, a_buf, b_buf, in_sem, out_sem):
    size = a_ref.shape[0] // pieces
    cuts = [pl.ds(i * size, size) for i in range(pieces)]
    moves = [(a_ref.at[cut], a_buf.at[cut], a_out.at[cut]) for cut in cuts]
    moves.append((b_ref, b_buf, b_out))
    loads = [
        pltpu.make_async_copy(src, buf, in_sem.at[i]) for i, (src, buf, _) in enumerate(moves)
    ]
    stores = [
        pltpu.make_async_copy(buf, dst, out_sem.at[i]) for i, (_, buf, dst) in enumerate(moves)
    ]
    for load in loads:
        load.start()
    for load, store in zip(loads, stores):
        load.wait()
        store.start()
    for store in stores:
        store.wait()


def local(
    queries,
    keys,
    values,
    out_gate,
    in_gate,
    forget_gate,
    out_gain,
    out_weight,
    moe_rows,
    moe_gain,
    routes,
    route_weight,
    expert_gate,
    expert_up,
    expert_down,
    shared_gate,
    shared_up,
    shared_down,
):
    tp_count = lax.axis_size("tp")
    ep_count = lax.axis_size("ep")
    count, depth = moe_rows.shape
    assert expert_gate.shape[0] == 1
    cap = 3 * count * routes.shape[1] // (2 * ep_count)
    slots = ep_count * cap
    heads = in_gate.shape[0]
    tok = queries.shape[0]
    held = heads * DK
    extra = -(-(1 + 2 * heads) // 8) * 8
    chips = tp_count // 2
    units, common = expert_gate.shape[2], shared_gate.shape[1]
    wide, features = out_weight.shape
    feat = features // tp_count
    share = wide // ep_count
    half = depth // 2
    side = 1
    while side * side < ep_count:
        side *= 2
    dma = pltpu.SemaphoreType.DMA

    def vm(*shape, dtype=BF16):
        return pltpu.VMEM(shape, dtype)

    scratch = [
        vm(ep_count, held + extra, 128, dtype=F32),
        vm(tok, heads * DV),
        vm(tp_count, tok, heads * DV),
        vm(tp_count, ep_count, share, feat),
        vm(tok, feat),
        vm(count, depth),
        vm(tok, held),
        vm(tok, held),
        vm(tok, heads * DV),
        vm(tok, heads * DV),
        vm(count, depth),
        vm(2, ep_count, cap, half),
        vm(2, ep_count, cap, half),
        vm(depth, units),
        vm(depth, units),
        vm(units, depth),
        vm(depth, common),
        vm(depth, common),
        vm(common, depth),
        vm(slots, units),
        vm(count, common),
        vm(chips, slots + count, feat),
        vm(chips, slots + count, feat),
        vm(chips, ep_count, cap, feat),
        vm(chips, ep_count, cap, feat),
        vm(chips, count, feat, dtype=F32),
        vm(chips, count, feat),
        vm(chips, count, feat),
        vm(count, feat, dtype=F32),
        vm(count, feat),
        dma((13,)),
        dma((2, -(-tok // 256))),
    ]
    scratch += [dma((tp_count,))] * 2
    scratch += [dma((SPLIT, ep_count))] * 2
    scratch += [dma((2, ep_count, ep_count)), dma((2, SPLIT, ep_count))]
    scratch += [dma((ep_count,))] * 2
    scratch += [dma((2, ep_count))] * 2
    scratch += [dma((ep_count,))] * 2
    scratch += [dma((SPLIT, chips))] * 6
    scratch += [dma((chips,))] * 2
    scratch += [dma((SPLIT, ep_count))] * 2
    scratch += [dma((chips,))] * 2
    mixer_sum, moe_sum = pl.pallas_call(
        functools.partial(step_kernel, ep_count, tp_count, side, cap),
        out_shape=(
            jax.ShapeDtypeStruct((tok, feat), BF16),
            jax.ShapeDtypeStruct((count, feat), BF16),
        ),
        in_specs=[VM] * 6 + [ANY] * 12,
        out_specs=(ANY, ANY),
        scratch_shapes=scratch,
        compiler_params=pltpu.CompilerParams(
            collective_id=0, has_side_effects=True, vmem_limit_bytes=60 * 1024 * 1024
        ),
        cost_estimate=pl.CostEstimate(
            flops=9_000_000_000, bytes_accessed=30_000_000, transcendentals=0
        ),
    )(
        in_gate,
        forget_gate,
        out_gain.reshape(1, -1),
        moe_gain.reshape(1, -1),
        routes.T,
        route_weight.T,
        queries,
        keys,
        values,
        out_gate,
        moe_rows,
        out_weight,
        expert_gate,
        expert_up,
        expert_down,
        shared_gate,
        shared_up,
        shared_down,
    )
    pieces = 4
    return pl.pallas_call(
        functools.partial(hand_over, pieces),
        out_shape=(
            jax.ShapeDtypeStruct((tok, feat), BF16),
            jax.ShapeDtypeStruct((count, feat), BF16),
        ),
        in_specs=[ANY] * 2,
        out_specs=(ANY, ANY),
        scratch_shapes=[
            vm(tok, feat),
            vm(count, feat),
            dma((pieces + 1,)),
            dma((pieces + 1,)),
        ],
    )(mixer_sum, moe_sum)


def solution(mesh):
    return jax.shard_map(
        local,
        mesh=mesh,
        in_specs=(
            P("ep", "tp"),
            P("ep", "tp"),
            P("ep", "tp"),
            P("ep", "tp"),
            P("tp", "ep"),
            P("tp", "ep"),
            P("tp"),
            P("tp", None),
            P("ep", None),
            P(),
            P("ep", None),
            P("ep", None),
            P("ep", None, "tp"),
            P("ep", None, "tp"),
            P("ep", "tp", None),
            P(None, "tp"),
            P(None, "tp"),
            P("tp", None),
        ),
        out_specs=(P("ep", "tp"), P("ep", "tp")),
        check_vma=False,
    )
```
